32 devices in a mesh: grp: 2 (over x), sp: 8 (over z, y), tp: 2 (over core).
Axes of the slice: x: 2, y: 2, z: 4, core: 2. Of those that a mesh axis runs over, the one named last changes fastest.
Arguments:
- tokens: bfloat16 [8192, 2048], P(('grp', 'sp', 'tp')), parts along dimension 0, may hold values from -64 to 64
- w_query: bfloat16 [2048, 1024], P(None, 'tp'), may hold values from -0.125 to 0.125
- w_key: bfloat16 [2048, 1024], P(None, 'tp'), may hold values from -0.125 to 0.125
- w_value: bfloat16 [2048, 1024], P(None, 'tp'), may hold values from -0.25 to 0.25
- w_out: bfloat16 [1024, 2048], P('tp'), may hold values from -0.1875 to 0.1875
Outputs:
- mixed: bfloat16 [8192, 2048], P(('grp', 'sp', 'tp')), parts along dimension 0
- log_sums: float32 [16, 8192], P('tp', ('grp', 'sp')), parts along dimension 1
The draws below stay inside these ranges and needn't reach their ends.
There are 2 independent parts, one for each index of `grp`. The reference program is written for one: setup_inputs(seed, part) draws one part's arguments, and reference() takes and returns one part's arrays. A program takes and returns all parts, laid end to end along the dimension named above; an argument that names none is the same for every part. Nothing has to cross between parts.
All inputs are finite; a program needn't handle non-finite values.
Results may differ from the reference program's by a relative error of at most 0.013.
The reference program's roundings to bfloat16 on the way count: a program that leaves them out, or rounds other values in their place, can miss the bound.
Values may be sent and summed in bfloat16 or wider, within the bound.
No kernel may reach another device: no remote copies, remote signals or barrier semaphores. Data moves between devices by JAX's collectives and lax.ppermute only.
A program may use at most 128 MiB of HBM per device.

```python
import math
import jax
import jax.numpy as jnp
from jax import lax

D = 2048
HEADS = 16
HEAD_DIM = 64
WINDOW_KEY_STEPS = 128
MIDDLE_DILATION = 4
FAR_DILATION = 16
TOK_DEV = 512
TOKENS = 4096
REACH = 2048
N_SP = 8
N_TP = 2


def draw_tokens(key, part):
    base = jnp.clip(jax.random.normal(jax.random.fold_in(key, 11), (TOKENS, D), jnp.float32), -4.0, 4.0)
    return base.astype(jnp.bfloat16)


def block_levels(own_key, dims, split, least, largest):
    loudness = 1.0
    for position, shards_of in split:
        steps = jax.random.uniform(jax.random.fold_in(jax.random.fold_in(own_key, 6), position), (shards_of,), jnp.float32, least / len(split), largest / len(split))
        loudness = loudness * jnp.repeat(jnp.exp(steps), dims[position] // shards_of).reshape((-1,) + (1,) * (len(dims) - 1 - position))
    return loudness


def bell_draw(key, dims, scale, bound, split=(), kind=jnp.bfloat16):
    result = scale * jax.random.normal(key, dims, jnp.float32)
    if split:
        result = result * block_levels(key, dims, split, -0.22, 0.18)
    return jnp.clip(result, -bound, bound).astype(kind)


def setup_inputs(seed: int = 0, part: int = 0) -> dict:
    key_list = jax.random.split(jax.random.key(seed), 6)
    part_splits = jax.random.split(jax.random.fold_in(key_list[5], part), 6)
    tokens = draw_tokens(jax.random.fold_in(jax.random.fold_in(key_list[5], part), 71), part)
    w_query = bell_draw(key_list[1], (D, HEADS * HEAD_DIM), D ** -0.5, 0.125, ((1, 2),))
    w_key = bell_draw(key_list[2], (D, HEADS * HEAD_DIM), D ** -0.5, 0.125, ((1, 2),))
    w_value = bell_draw(key_list[3], (D, HEADS * HEAD_DIM), (D // 4) ** -0.5, 0.25, ((1, 2),))
    w_out = bell_draw(key_list[4], (HEADS * HEAD_DIM, D), (HEADS * HEAD_DIM) ** -0.5, 0.1875, ((0, 2),))
    return dict(tokens=tokens, w_query=w_query, w_key=w_key, w_value=w_value, w_out=w_out)


ALIBI_EXP = 16.0


def dilated_attention(query_rows, key_value_rows, dilation, window_steps, head_slopes, first_position):
    length, heads, depth = query_rows.shape
    total_rows = key_value_rows.shape[0]
    strided = length // dilation
    block_rows = math.gcd(strided, 128)
    num_blocks = strided // block_rows
    behind = (total_rows - length) // dilation
    grouped = query_rows.reshape(num_blocks, block_rows, dilation, heads, depth)
    columns = key_value_rows.reshape(total_rows // dilation, dilation, 2, heads, depth)
    spans = jnp.stack([columns[behind + index * block_rows - window_steps: behind + (index + 1) * block_rows]
                       for index in range(num_blocks)])
    scores = jnp.einsum("bqrhe,bkrhe->brhqk", grouped.astype(jnp.float32),
                        spans[:, :, :, 0].astype(jnp.float32)) * depth ** -0.5
    row_pos = jnp.arange(block_rows, dtype=jnp.int32)[:, None]
    key_pos = jnp.arange(window_steps + block_rows, dtype=jnp.int32)[None, :]
    distance = window_steps + row_pos - key_pos
    inside = (distance >= 0) & (distance <= window_steps)
    block_pos = jnp.arange(num_blocks, dtype=jnp.int32)[:, None, None, None]
    residue = jnp.arange(dilation, dtype=jnp.int32)[None, :, None, None]
    source = first_position + (block_pos * block_rows - window_steps + key_pos[None, None]) * dilation + residue
    allowed = inside[None, None] & (source >= 0)
    penalty = -head_slopes[:, None, None] * (distance * dilation).astype(jnp.float32)
    scores = jnp.where(allowed[:, :, None], scores + penalty[None, None], -jnp.inf)
    maxima = jnp.max(scores, axis=-1, keepdims=True)
    weights = jnp.exp(scores - maxima)
    totals = jnp.sum(weights, axis=-1, keepdims=True)
    rounded = lax.optimization_barrier(weights.astype(jnp.bfloat16))
    summed = jnp.einsum("brhqk,bkrhe->bqrhe", rounded.astype(jnp.float32), spans[:, :, :, 1].astype(jnp.float32))
    outputs = summed / jnp.transpose(totals, (0, 3, 1, 2, 4))
    log_part = jnp.transpose((maxima + jnp.log(totals))[..., 0], (0, 3, 1, 2))
    return outputs.reshape(length, heads, depth), log_part.reshape(length, heads)


def combine(query_rows, key_value_rows, head_slopes, first_position):
    length, heads, depth = query_rows.shape
    window_results = [dilated_attention(query_rows, key_value_rows, window_stride, WINDOW_KEY_STEPS, head_slopes, first_position) for window_stride in (1, MIDDLE_DILATION, FAR_DILATION)]
    stacked = jnp.stack([item[1] for item in window_results])
    log_total = jax.nn.logsumexp(stacked, axis=0)
    hidden = jnp.zeros((length, heads, depth), jnp.float32)
    for item in window_results:
        hidden = hidden + jnp.exp(item[1] - log_total)[..., None] * item[0]
    return hidden.reshape(length, heads * depth).astype(jnp.bfloat16), log_total


def reference(tokens, w_query, w_key, w_value, w_out):
    query_rows = jnp.dot(tokens, w_query, preferred_element_type=jnp.float32).astype(jnp.bfloat16)
    keys = jnp.dot(tokens, w_key, preferred_element_type=jnp.float32).astype(jnp.bfloat16)
    values = jnp.dot(tokens, w_value, preferred_element_type=jnp.float32).astype(jnp.bfloat16)
    key_value_rows = jnp.concatenate([keys, values], axis=1)
    padded = jnp.concatenate([jnp.zeros((REACH, key_value_rows.shape[1]), jnp.bfloat16), key_value_rows], axis=0)
    head_slopes = jnp.exp2(-ALIBI_EXP * jnp.arange(1, HEADS + 1, dtype=jnp.float32) / HEADS)

    def segment(index):
        first = index * TOK_DEV
        query_seg = lax.dynamic_slice_in_dim(query_rows, first, TOK_DEV, 0).reshape(TOK_DEV, HEADS, HEAD_DIM)
        keyval_seg = lax.dynamic_slice_in_dim(padded, first, REACH + TOK_DEV, 0)
        return combine(query_seg, keyval_seg, head_slopes, first)

    hidden, log_total = lax.map(segment, jnp.arange(N_SP, dtype=jnp.int32))
    hidden = hidden.reshape(TOKENS, HEADS * HEAD_DIM)
    log_total = log_total.reshape(TOKENS, HEADS)
    width = HEADS * HEAD_DIM // N_TP
    mixed = jnp.zeros((TOKENS, D), jnp.float32)
    for group in range(N_TP):
        partial_value = jnp.dot(hidden[:, group * width:(group + 1) * width], w_out[group * width:(group + 1) * width],
                          preferred_element_type=jnp.float32).astype(jnp.bfloat16)
        mixed = mixed + lax.optimization_barrier(partial_value).astype(jnp.float32)
    return mixed.astype(jnp.bfloat16), log_total.T
```

```python
import functools
import math

import jax
import jax.numpy as jnp
from jax import lax
from jax.experimental import pallas as pl
from jax.experimental.pallas import tpu as pltpu
from jax.sharding import PartitionSpec as P

HEADS = 16
HEAD_DIM = 64
WINDOW_KEY_STEPS = 128
MIDDLE_DILATION = 4
FAR_DILATION = 16
REACH = 2048
ALIBI_EXP = 16.0

LOG2E = math.log2(math.e)
LN2 = math.log(2.0)
MASKED = -1e30
FLOOR = -1e25
F32 = jnp.float32
BF16 = jnp.bfloat16
ANY = pl.BlockSpec(memory_space=pl.ANY)
SMEM = pl.BlockSpec(memory_space=pltpu.SMEM)
VMEM = pl.BlockSpec(memory_space=pltpu.VMEM)
PARAMS = pltpu.CompilerParams(vmem_limit_bytes=56 * 1024 * 1024)

SUB = 16


def aligned(value, multiple):
    return value if isinstance(value, int) else pl.multiple_of(value, multiple)


def copy_all(pairs, sems):
    copies = [pltpu.make_async_copy(s, d, sems.at[n]) for n, (s, d) in enumerate(pairs)]
    for item in copies:
        item.start()
    return copies


def project_kernel(lanes, meta, x_own, x_other, w_q, w_k, w_v, kv_out, q_out, xs, ws, acc, sems):
    side, tp = meta[0], meta[1]
    rows = xs.shape[1]
    columns = pl.ds(aligned(side * lanes, lanes), lanes)
    copies = copy_all(
        [
            (x_own, xs.at[0]),
            (w_k.at[:, columns], ws.at[0]),
            (w_v.at[:, columns], ws.at[1]),
            (x_other, xs.at[1]),
            (w_q.at[:, columns], ws.at[2]),
        ],
        sems,
    )
    copies[0].wait()
    for which in range(3):
        copies[(1, 2, 4)[which]].wait()
        for half in range(2):
            if which == 0 and half == 1:
                copies[3].wait()
            result = jnp.dot(xs[half], ws[which], preferred_element_type=F32)
            for part in range(lanes // 128):
                acc[part] = result[:, part * 128 : (part + 1) * 128]
            place = (tp if half == 0 else 1 - tp) * rows
            for residue in range(FAR_DILATION):
                for part in range(lanes // 128):
                    chunk = acc[part, pl.ds(residue, SUB, stride=FAR_DILATION), :].astype(BF16)
                    target = pl.ds(aligned(place + residue * SUB, SUB), SUB)
                    if which < 2:
                        start = which * lanes + part * 128
                        kv_out[target, start : start + 128] = chunk
                    else:
                        q_out[target, part * 128 : (part + 1) * 128] = chunk


def project(meta, x_own, x_other, w_q, w_k, w_v, lanes):
    rows, width = x_own.shape
    return pl.pallas_call(
        functools.partial(project_kernel, lanes),
        out_shape=[
            jax.ShapeDtypeStruct((2 * rows, 2 * lanes), BF16),
            jax.ShapeDtypeStruct((2 * rows, lanes), BF16),
        ],
        in_specs=[SMEM] + [ANY] * 5,
        out_specs=[VMEM, VMEM],
        scratch_shapes=[
            pltpu.VMEM((2, rows, width), BF16),
            pltpu.VMEM((3, width, lanes), BF16),
            pltpu.VMEM((lanes // 128, rows, 128), F32),
            pltpu.SemaphoreType.DMA((5,)),
        ],
        compiler_params=PARAMS,
        cost_estimate=pl.CostEstimate(
            flops=2 * 2 * rows * width * 3 * lanes,
            bytes_accessed=2 * width * (2 * rows + 3 * lanes),
            transcendentals=0,
        ),
        name="project",
    )(meta, x_own, x_other, w_q, w_k, w_v)


def attend(queries, keys, values, bias):
    rows = queries.shape[0]
    low = lax.broadcasted_iota(jnp.int32, (rows, 128), 1) < HEAD_DIM
    zero = jnp.zeros_like(queries)
    stacked = jnp.concatenate([jnp.where(low, queries, zero), jnp.where(low, zero, queries)], axis=0)
    scores = lax.dot_general(
        stacked, keys, (((1,), (1,)), ((), ())), preferred_element_type=F32
    )
    scores = scores * (HEAD_DIM**-0.5 * LOG2E) + bias
    maxima = jnp.maximum(jnp.max(scores, axis=1, keepdims=True), FLOOR)
    weights = jnp.exp2(scores - maxima)
    totals = jnp.sum(weights, axis=1, keepdims=True)
    summed = jnp.dot(weights.astype(BF16), values, preferred_element_type=F32)
    pick = lambda item: jnp.where(low, item[:rows], item[rows:])
    return pick(summed), pick(maxima), pick(totals)


def merge(first, second):
    o1, m1, l1 = first
    o2, m2, l2 = second
    top = jnp.maximum(m1, m2)
    a, b = jnp.exp2(m1 - top), jnp.exp2(m2 - top)
    return o1 * a + o2 * b, top, l1 * a + l2 * b


def near_distance(keys_before, keys_own):
    tile = FAR_DILATION * SUB
    token = lambda n: FAR_DILATION * (n % SUB) + n // SUB
    shape = (tile, (tile if keys_before else 0) + (tile if keys_own else 0))
    row = token(lax.broadcasted_iota(jnp.int32, shape, 0))
    col = lax.broadcasted_iota(jnp.int32, shape, 1)
    if keys_before:
        key = jnp.where(col < tile, token(col) - tile, token(col - tile))
    else:
        key = token(col)
    return row - key


def middle_distance(keys_before, keys_own, chunks):
    group = FAR_DILATION // MIDDLE_DILATION
    size = chunks * group * SUB
    step = lambda n: (n // (group * SUB)) * (group * SUB) + group * (n % SUB) + (n // SUB) % group
    shape = (size, (size if keys_before else 0) + (size if keys_own else 0))
    row = step(lax.broadcasted_iota(jnp.int32, shape, 0))
    col = lax.broadcasted_iota(jnp.int32, shape, 1)
    if keys_before:
        key = jnp.where(col < size, step(col) - size, step(col - size))
    else:
        key = step(col)
    return row - key


def bias_of(distance, slope, stride):
    allowed = (distance >= 0) & (distance <= WINDOW_KEY_STEPS)
    return jnp.where(allowed, distance.astype(F32) * (slope * (-float(stride))), MASKED)


def rows_of(ref, starts, lanes):
    return jnp.concatenate([ref[pl.ds(aligned(s, SUB), SUB), lanes] for s in starts], axis=0)


def middle_starts(block, residue, chunks):
    tile = FAR_DILATION * SUB
    group = FAR_DILATION // MIDDLE_DILATION
    return [
        (block * chunks + s) * tile + (residue + MIDDLE_DILATION * b) * SUB
        for s in range(chunks)
        for b in range(group)
    ]


def far_starts(residue, chunks):
    return [g * FAR_DILATION * SUB + residue * SUB for g in range(chunks)]


def fold_in(refs, starts, lanes, new):
    size = SUB
    for n, start in enumerate(starts):
        where = (pl.ds(aligned(start, SUB), size), lanes)
        old = tuple(ref[where] for ref in refs)
        piece = tuple(item[n * size : (n + 1) * size] for item in new)
        for ref, value in zip(refs, merge(old, piece)):
            ref[where] = value


def pair_lanes(pair, offset=0):
    return slice(offset + pair * 128, offset + (pair + 1) * 128)


def local_kernel(meta, slopes, q_mine, q_part, kv_mine, kv_part, o_ref, m_ref, l_ref, q, kv, near, mid, sems):
    y = meta[2]
    block, lanes = q_mine.shape
    pairs = lanes // 128
    tile = FAR_DILATION * SUB
    chunks = block // tile
    mine = pl.ds(aligned(y * block, block), block)
    part = pl.ds(aligned((1 - y) * block, block), block)
    copies = copy_all(
        [(q_mine, q.at[mine]), (q_part, q.at[part]), (kv_mine, kv.at[mine]), (kv_part, kv.at[part])],
        sems,
    )
    distance = near_distance(True, True)
    for head in range(2 * pairs):
        near[head] = bias_of(distance, slopes[head], 1)
    distance = middle_distance(True, True, chunks)
    for head in range(2 * pairs):
        mid[head] = bias_of(distance, slopes[head], MIDDLE_DILATION)
    for item in copies:
        item.wait()
    refs = (o_ref, m_ref, l_ref)
    step = 64
    per_tile = tile // step

    def near_step(tile_index, inner, before):
        start = aligned(tile_index * tile + inner * step, step)
        first = aligned((tile_index - 1) * tile if before else tile_index * tile, tile)
        count = 2 * tile if before else tile
        for pair in range(pairs):
            select = pl.ds(aligned(inner * step, step), step)
            columns = slice(0, 2 * tile) if before else slice(tile, 2 * tile)
            bias = jnp.concatenate(
                [near[2 * pair, select, columns], near[2 * pair + 1, select, columns]], axis=0
            )
            result = attend(
                q[pl.ds(start, step), pair_lanes(pair)],
                kv[pl.ds(first, count), pair_lanes(pair)],
                kv[pl.ds(first, count), pair_lanes(pair, lanes)],
                bias,
            )
            for ref, value in zip(refs, result):
                ref[pl.ds(start, step), pair_lanes(pair)] = value

    @pl.loop(0, per_tile)
    def _(n):
        near_step(0, n, False)

    @pl.loop(0, (2 * chunks - 1) * per_tile)
    def _(n):
        near_step(1 + n // per_tile, n % per_tile, True)

    size = mid.shape[1]

    @pl.loop(0, MIDDLE_DILATION)
    def _(residue):
        for index in range(2):
            starts = middle_starts(index, residue, chunks)
            key_starts = (middle_starts(0, residue, chunks) if index else []) + starts
            columns = slice(0, 2 * size) if index else slice(size, 2 * size)
            for pair in range(pairs):
                bias = jnp.concatenate([mid[2 * pair, :, columns], mid[2 * pair + 1, :, columns]], axis=0)
                result = attend(
                    rows_of(q, starts, pair_lanes(pair)),
                    rows_of(kv, key_starts, pair_lanes(pair)),
                    rows_of(kv, key_starts, pair_lanes(pair, lanes)),
                    bias,
                )
                fold_in(refs, starts, pair_lanes(pair), result)


def local_attention(meta, slopes, q_mine, q_part, kv_mine, kv_part):
    block, lanes = q_mine.shape
    tile = FAR_DILATION * SUB
    state = jax.ShapeDtypeStruct((2 * block, lanes), F32)
    heads = lanes // HEAD_DIM
    size = block // MIDDLE_DILATION
    return pl.pallas_call(
        local_kernel,
        out_shape=[state] * 3,
        in_specs=[SMEM, SMEM] + [ANY] * 4,
        out_specs=[VMEM] * 3,
        scratch_shapes=[
            pltpu.VMEM((2 * block, lanes), BF16),
            pltpu.VMEM((2 * block, 2 * lanes), BF16),
            pltpu.VMEM((heads, tile, 2 * tile), F32),
            pltpu.VMEM((heads, size, 2 * size), F32),
            pltpu.SemaphoreType.DMA((4,)),
        ],
        compiler_params=PARAMS,
        cost_estimate=pl.CostEstimate(flops=4 * 10**9, bytes_accessed=4 * 10**6, transcendentals=0),
        name="local",
    )(meta, slopes, q_mine, q_part, kv_mine, kv_part)


def before_kernel(
    meta, slopes, gate, q_mine, q_part, kv_mine, kv_part, kv_a, kv_b, o_in, m_in, l_in,
    o_ref, m_ref, l_ref, q, kv, past, near, mid, far, sems,
):
    y = meta[2]
    block, lanes = q_mine.shape
    pairs = lanes // 128
    tile = FAR_DILATION * SUB
    chunks = block // tile
    mine = pl.ds(aligned(y * block, block), block)
    part = pl.ds(aligned((1 - y) * block, block), block)
    copies = copy_all(
        [
            (q_mine, q.at[mine]), (q_part, q.at[part]), (kv_mine, kv.at[mine]), (kv_part, kv.at[part]),
            (kv_a, past.at[mine]), (kv_b, past.at[part]),
            (o_in, o_ref), (m_in, m_ref), (l_in, l_ref),
        ],
        sems,
    )
    closed = gate[0]
    size = mid.shape[1]
    row = lax.broadcasted_iota(jnp.int32, far.shape[1:], 0)
    col = lax.broadcasted_iota(jnp.int32, far.shape[1:], 1)
    half = far.shape[2] // 2
    steps = row - col + half
    for head in range(2 * pairs):
        far[head] = bias_of(steps, slopes[head], FAR_DILATION) + jnp.where(col < half, closed, 0.0)
        near[head] = bias_of(near_distance(True, False), slopes[head], 1) + closed
        mid[head] = bias_of(middle_distance(True, False, chunks), slopes[head], MIDDLE_DILATION) + closed
    for item in copies:
        item.wait()
    refs = (o_ref, m_ref, l_ref)

    @pl.loop(0, FAR_DILATION)
    def _(residue):
        starts = far_starts(residue, 2 * chunks)
        for pair in range(pairs):
            keys = [rows_of(ref, starts, pair_lanes(pair)) for ref in (past, kv)]
            values = [rows_of(ref, starts, pair_lanes(pair, lanes)) for ref in (past, kv)]
            result = attend(
                rows_of(q, starts, pair_lanes(pair)),
                jnp.concatenate(keys, axis=0),
                jnp.concatenate(values, axis=0),
                jnp.concatenate([far[2 * pair], far[2 * pair + 1]], axis=0),
            )
            fold_in(refs, starts, pair_lanes(pair), result)

    step = 64
    last = (2 * chunks - 1) * tile

    @pl.loop(0, tile // step)
    def _(n):
        select = pl.ds(aligned(n * step, step), step)
        for pair in range(pairs):
            result = attend(
                q[select, pair_lanes(pair)],
                past[last : last + tile, pair_lanes(pair)],
                past[last : last + tile, pair_lanes(pair, lanes)],
                jnp.concatenate([near[2 * pair, select], near[2 * pair + 1, select]], axis=0),
            )
            old = tuple(ref[select, pair_lanes(pair)] for ref in refs)
            for ref, value in zip(refs, merge(old, result)):
                ref[select, pair_lanes(pair)] = value

    @pl.loop(0, MIDDLE_DILATION)
    def _(residue):
        starts = middle_starts(0, residue, chunks)
        key_starts = middle_starts(1, residue, chunks)
        for pair in range(pairs):
            result = attend(
                rows_of(q, starts, pair_lanes(pair)),
                rows_of(past, key_starts, pair_lanes(pair)),
                rows_of(past, key_starts, pair_lanes(pair, lanes)),
                jnp.concatenate([mid[2 * pair], mid[2 * pair + 1]], axis=0),
            )
            fold_in(refs, starts, pair_lanes(pair), result)


def before_attention(meta, slopes, gate, q_mine, q_part, kv_mine, kv_part, kv_a, kv_b, state):
    block, lanes = q_mine.shape
    tile = FAR_DILATION * SUB
    shape = jax.ShapeDtypeStruct((2 * block, lanes), F32)
    heads = lanes // HEAD_DIM
    size = block // MIDDLE_DILATION
    reach = 2 * block // FAR_DILATION
    return pl.pallas_call(
        before_kernel,
        out_shape=[shape] * 3,
        in_specs=[SMEM, SMEM, SMEM] + [ANY] * 9,
        out_specs=[VMEM] * 3,
        scratch_shapes=[
            pltpu.VMEM((2 * block, lanes), BF16),
            pltpu.VMEM((2 * block, 2 * lanes), BF16),
            pltpu.VMEM((2 * block, 2 * lanes), BF16),
            pltpu.VMEM((heads, tile, tile), F32),
            pltpu.VMEM((heads, size, size), F32),
            pltpu.VMEM((heads, reach, 2 * reach), F32),
            pltpu.SemaphoreType.DMA((9,)),
        ],
        compiler_params=PARAMS,
        cost_estimate=pl.CostEstimate(flops=2 * 10**9, bytes_accessed=4 * 10**6, transcendentals=0),
        name="before",
    )(meta, slopes, gate, q_mine, q_part, kv_mine, kv_part, kv_a, kv_b, *state)


def selector(lanes, part):
    shape = (16, lanes)
    row = lax.broadcasted_iota(jnp.int32, shape, 0)
    lane = lax.broadcasted_iota(jnp.int32, shape, 1)
    heads = lanes // HEAD_DIM
    return jnp.where((row // heads == part) & (lane == (row % heads) * HEAD_DIM), 1.0, 0.0).astype(BF16)


def spreader(lanes):
    shape = (16, lanes)
    row = lax.broadcasted_iota(jnp.int32, shape, 0)
    lane = lax.broadcasted_iota(jnp.int32, shape, 1)
    heads = lanes // HEAD_DIM
    return jnp.where((row < 3 * heads) & (lane // HEAD_DIM == row % heads), 1.0, 0.0).astype(BF16)


def pack_sums(sums):
    lanes = sums.shape[1]
    total = jnp.zeros((16, sums.shape[0]), F32)
    for part in range(3):
        piece = sums.astype(BF16)
        sums = sums - piece.astype(F32)
        total = total + lax.dot_general(
            selector(lanes, part), piece, (((1,), (1,)), ((), ())), preferred_element_type=F32
        )
    return total.astype(BF16)


def unpack_sums(packed, lanes):
    return lax.dot_general(packed, spreader(lanes), (((0,), (0,)), ((), ())), preferred_element_type=F32)


def remote_kernel(meta, slopes, gate, q_a, q_b, kv_a, kv_b, own_ref, other_ref, q, kv, far, out, sums, sems):
    y = meta[2]
    block, lanes = q_a.shape
    pairs = lanes // 128
    tile = FAR_DILATION * SUB
    chunks = block // tile
    mine = pl.ds(aligned(y * block, block), block)
    part = pl.ds(aligned((1 - y) * block, block), block)
    copies = copy_all(
        [(q_a, q.at[mine]), (q_b, q.at[part]), (kv_a, kv.at[mine]), (kv_b, kv.at[part])], sems
    )
    closed = gate[0]
    row = lax.broadcasted_iota(jnp.int32, far.shape[1:], 0)
    col = lax.broadcasted_iota(jnp.int32, far.shape[1:], 1)
    steps = row - col + 2 * far.shape[2]
    for head in range(2 * pairs):
        far[head] = bias_of(steps, slopes[head], FAR_DILATION) + closed
    for item in copies:
        item.wait()

    @pl.loop(0, FAR_DILATION)
    def _(residue):
        starts = far_starts(residue, 2 * chunks)
        for pair in range(pairs):
            o, m, l = attend(
                rows_of(q, starts, pair_lanes(pair)),
                rows_of(kv, starts, pair_lanes(pair)),
                rows_of(kv, starts, pair_lanes(pair, lanes)),
                jnp.concatenate([far[2 * pair], far[2 * pair + 1]], axis=0),
            )
            some = l > 0.0
            safe = jnp.where(some, l, 1.0)
            o = o / safe
            s = jnp.where(some, m + jnp.log2(safe), FLOOR)
            for n, start in enumerate(starts):
                where = (pl.ds(aligned(start, SUB), SUB), pair_lanes(pair))
                out[where] = o[n * SUB : (n + 1) * SUB].astype(BF16)
                sums[where] = s[n * SUB : (n + 1) * SUB]

    for select, ref in ((mine, own_ref), (part, other_ref)):
        ref[:block] = out[select]
        packed = pack_sums(sums[select])
        for n in range(block // lanes):
            ref[block + 16 * n : block + 16 * (n + 1)] = packed[:, n * lanes : (n + 1) * lanes]


def remote_attention(meta, slopes, gate, q_a, q_b, kv_a, kv_b):
    block, lanes = q_a.shape
    heads = lanes // HEAD_DIM
    reach = 2 * block // FAR_DILATION
    shape = jax.ShapeDtypeStruct((block + 16 * (block // lanes), lanes), BF16)
    return pl.pallas_call(
        remote_kernel,
        out_shape=[shape] * 2,
        in_specs=[SMEM, SMEM, SMEM] + [ANY] * 4,
        out_specs=[VMEM] * 2,
        scratch_shapes=[
            pltpu.VMEM((2 * block, lanes), BF16),
            pltpu.VMEM((2 * block, 2 * lanes), BF16),
            pltpu.VMEM((heads, reach, reach), F32),
            pltpu.VMEM((2 * block, lanes), BF16),
            pltpu.VMEM((2 * block, lanes), F32),
            pltpu.SemaphoreType.DMA((4,)),
        ],
        compiler_params=PARAMS,
        cost_estimate=pl.CostEstimate(flops=10**9, bytes_accessed=2 * 10**6, transcendentals=0),
        name="remote",
    )(meta, slopes, gate, q_a, q_b, kv_a, kv_b)


def finish_kernel(meta, gate, o_in, m_in, l_in, far_in, stay_ref, go_ref, o_s, m_s, l_s, turned, sems):
    which, tp = meta[0], meta[1]
    block, lanes = o_s.shape
    tile = FAR_DILATION * SUB
    chunks = block // tile
    select = pl.ds(aligned(which * block, block), block)
    copies = copy_all(
        [(o_in.at[select], o_s), (m_in.at[select], m_s), (l_in.at[select], l_s)], sems
    )
    for item in copies:
        item.wait()
    per = lanes // tile
    for s in range(chunks):
        rows = slice(s * tile, (s + 1) * tile)
        packed = far_in[block + 16 * (s // per) : block + 16 * (s // per) + 16, (s % per) * tile : (s % per + 1) * tile]
        far_sums = unpack_sums(packed, lanes) + gate[0]
        o, m, l = merge(
            (o_s[rows], m_s[rows], l_s[rows]),
            (far_in[rows].astype(F32), far_sums, jnp.ones_like(far_sums)),
        )
        o_s[rows] = o / l
        m_s[rows] = (m + jnp.log2(l)) * LN2
    for item, ref in enumerate((o_s, m_s)):
        for s in range(chunks):
            for residue in range(FAR_DILATION):
                for part in range(lanes // 128):
                    turned[item, part, pl.ds(s * tile + residue, SUB, stride=FAR_DILATION), :] = ref[
                        s * tile + residue * SUB : s * tile + (residue + 1) * SUB, part * 128 : (part + 1) * 128
                    ]
    half = block // 2
    for part in range(lanes // 128):
        for ref, place in ((stay_ref, tp * half), (go_ref, (1 - tp) * half)):
            ref[:half, part * 128 : (part + 1) * 128] = turned[0, part, pl.ds(aligned(place, half), half), :].astype(BF16)
    sums = jnp.concatenate([turned[1, part] for part in range(lanes // 128)], axis=1)
    packed = pack_sums(sums)
    for n in range(block // lanes):
        stay_ref[half + 16 * n : half + 16 * (n + 1)] = packed[:, n * lanes : (n + 1) * lanes]


def finish(meta, gate, state, far):
    lanes = far.shape[1]
    block = state[0].shape[0] // 2
    half = block // 2
    return pl.pallas_call(
        finish_kernel,
        out_shape=[
            jax.ShapeDtypeStruct((half + 16 * (block // lanes), lanes), BF16),
            jax.ShapeDtypeStruct((half, lanes), BF16),
        ],
        in_specs=[SMEM, SMEM] + [ANY] * 3 + [VMEM],
        out_specs=[VMEM] * 2,
        scratch_shapes=[
            pltpu.VMEM((block, lanes), F32),
            pltpu.VMEM((block, lanes), F32),
            pltpu.VMEM((block, lanes), F32),
            pltpu.VMEM((2, lanes // 128, block, 128), F32),
            pltpu.SemaphoreType.DMA((3,)),
        ],
        compiler_params=PARAMS,
        cost_estimate=pl.CostEstimate(flops=5 * 10**8, bytes_accessed=2 * 10**6, transcendentals=0),
        name="finish",
    )(meta, gate, *state, far)


def output_kernel(meta, stay, same, tp_piece, cross, w_mine, w_other, out_ref, sums_ref):
    y = meta[2]
    half, width = out_ref.shape
    lanes = stay.shape[1]
    heads = lanes // HEAD_DIM
    block = 2 * half
    near_rows = pl.ds(aligned(y * lanes, lanes), lanes)
    far_rows = pl.ds(aligned((1 - y) * lanes, lanes), lanes)
    step = 512
    for start in range(0, width, step):
        columns = slice(start, start + step)
        first = jnp.dot(stay[:half], w_mine[near_rows, columns], preferred_element_type=F32)
        first += jnp.dot(same[:half], w_mine[far_rows, columns], preferred_element_type=F32)
        second = jnp.dot(tp_piece[...], w_other[near_rows, columns], preferred_element_type=F32)
        second += jnp.dot(cross[...], w_other[far_rows, columns], preferred_element_type=F32)
        out_ref[:, columns] = (first.astype(BF16).astype(F32) + second.astype(BF16).astype(F32)).astype(BF16)
    for ref, place in ((stay, y), (same, 1 - y)):
        for n in range(block // lanes):
            packed = ref[half + 16 * n : half + 16 * (n + 1)].astype(F32)
            total = packed[:heads] + packed[heads : 2 * heads] + packed[2 * heads : 3 * heads]
            sums_ref[place, :, n * lanes : (n + 1) * lanes] = total


def output(meta, stay, same, tp_piece, cross, w_mine, w_other):
    half, lanes = tp_piece.shape
    width = w_mine.shape[1]
    heads = lanes // HEAD_DIM
    return pl.pallas_call(
        output_kernel,
        out_shape=[
            jax.ShapeDtypeStruct((half, width), BF16),
            jax.ShapeDtypeStruct((2, heads, 2 * half), F32),
        ],
        in_specs=[SMEM] + [VMEM] * 6,
        out_specs=[VMEM] * 2,
        compiler_params=PARAMS,
        cost_estimate=pl.CostEstimate(
            flops=2 * half * width * 4 * lanes, bytes_accessed=6 * 10**6, transcendentals=0
        ),
        name="output",
    )(meta, stay, same, tp_piece, cross, w_mine, w_other)


def body(tokens, w_query, w_key, w_value, w_out):
    half, _ = tokens.shape
    block = 2 * half
    width = w_query.shape[1]
    lanes = width // 2
    count = lax.axis_size("sp")
    pair = 2
    assert lax.axis_size("tp") == 2 and count % pair == 0
    assert REACH == 2 * pair * block and half == FAR_DILATION * SUB and lanes % 128 == 0
    ahead = [(n, n + pair) for n in range(count - pair)]
    back = [(n + pair, n) for n in range(count - pair)]
    beside = [(n, n ^ 1) for n in range(count)]
    swap = [(0, 1), (1, 0)]
    crossed = [(2 * n + c, 2 * (n ^ 1) + 1 - c) for n in range(count) for c in range(2)]

    place = lax.axis_index("sp")
    y = place % 2
    z = place // 2
    tp = lax.axis_index("tp")
    meta_mine = jnp.stack([y, tp, y]).astype(jnp.int32)
    meta_other = jnp.stack([1 - y, tp, y]).astype(jnp.int32)
    heads = lanes // HEAD_DIM
    head_ids = tp * (2 * heads) + y * heads + jnp.arange(1, heads + 1, dtype=jnp.int32)
    slopes = jnp.exp2(-ALIBI_EXP * head_ids.astype(F32) / HEADS) * LOG2E
    gate = jnp.where(z > 0, 0.0, MASKED).astype(F32).reshape(1)

    x_other = lax.ppermute(tokens, "tp", swap)
    kv_t, q_t = project(meta_other, tokens, x_other, w_query, w_key, w_value, lanes)
    kv_m, q_m = project(meta_mine, tokens, x_other, w_query, w_key, w_value, lanes)
    kv_p = lax.ppermute(kv_t, "sp", beside)
    kv_a = lax.ppermute(kv_m, "sp", ahead)
    q_p = lax.ppermute(q_t, "sp", beside)
    q_a = lax.ppermute(q_m, "sp", back)
    kv_b = lax.ppermute(kv_p, "sp", ahead)
    q_b = lax.ppermute(q_p, "sp", back)
    w_other = lax.ppermute(w_out, "tp", swap)
    state = local_attention(meta_mine, slopes, q_m, q_p, kv_m, kv_p)
    far_own, far_other = remote_attention(meta_mine, slopes, gate, q_a, q_b, kv_a, kv_b)
    far_p = lax.ppermute(far_other, "sp", ahead)
    far_m = lax.ppermute(far_own, "sp", ahead)
    state = before_attention(meta_mine, slopes, gate, q_m, q_p, kv_m, kv_p, kv_a, kv_b, state)
    same_go, cross_go = finish(meta_other, gate, state, far_p)
    same = lax.ppermute(same_go, "sp", beside)
    cross = lax.ppermute(cross_go, ("sp", "tp"), crossed)
    stay, tp_go = finish(meta_mine, gate, state, far_m)
    tp_piece = lax.ppermute(tp_go, "tp", swap)
    mixed, sums = output(meta_mine, stay, same, tp_piece, cross, w_out, w_other)
    return mixed, sums.reshape(2 * heads, block)


def solution(mesh):
    in_specs = (
        P(("grp", "sp", "tp"), None),
        P(None, "tp"),
        P(None, "tp"),
        P(None, "tp"),
        P("tp", None),
    )
    out_specs = (P(("grp", "sp", "tp"), None), P("tp", ("grp", "sp")))
    return jax.shard_map(body, mesh=mesh, in_specs=in_specs, out_specs=out_specs, check_vma=False)
```

```python
import functools
import math

import jax
import jax.numpy as jnp
from jax import lax
from jax.experimental import pallas as pl
from jax.experimental.pallas import tpu as pltpu
from jax.sharding import PartitionSpec as P

HEADS = 16
HEAD_DIM = 64
WINDOW_KEY_STEPS = 128
MIDDLE_DILATION = 4
FAR_DILATION = 16
REACH = 2048
ALIBI_EXP = 16.0

LOG2E = math.log2(math.e)
LN2 = math.log(2.0)
MASKED = -1e30
FLOOR = -1e25
F32 = jnp.float32
BF16 = jnp.bfloat16
ANY = pl.BlockSpec(memory_space=pl.ANY)
SMEM = pl.BlockSpec(memory_space=pltpu.SMEM)
VMEM = pl.BlockSpec(memory_space=pltpu.VMEM)
MIB = 1024 * 1024


def params(limit):
    return pltpu.CompilerParams(vmem_limit_bytes=limit * MIB)


SUB = 16


def aligned(value, multiple):
    return value if isinstance(value, int) else pl.multiple_of(value, multiple)


def project_kernel(lanes, meta, x_own, x_other, w_q, w_k, w_v, kv_out, q_out, acc):
    side, tp = meta[0], meta[1]
    rows = x_own.shape[0]
    columns = pl.ds(aligned(side * lanes, lanes), lanes)
    for which, w in enumerate((w_k, w_v, w_q)):
        for half, x in enumerate((x_own, x_other)):
            result = jnp.dot(x[...], w[:, columns], preferred_element_type=F32)
            for part in range(lanes // 128):
                acc[part] = result[:, part * 128 : (part + 1) * 128]
            place = (tp if half == 0 else 1 - tp) * rows
            for residue in range(FAR_DILATION):
                for part in range(lanes // 128):
                    chunk = acc[part, pl.ds(residue, SUB, stride=FAR_DILATION), :].astype(BF16)
                    target = pl.ds(aligned(place + residue * SUB, SUB), SUB)
                    if which < 2:
                        start = which * lanes + part * 128
                        kv_out[target, start : start + 128] = chunk
                    else:
                        q_out[target, part * 128 : (part + 1) * 128] = chunk


def project(meta, x_own, x_other, w_q, w_k, w_v, lanes):
    rows, width = x_own.shape
    return pl.pallas_call(
        functools.partial(project_kernel, lanes),
        out_shape=[
            jax.ShapeDtypeStruct((2 * rows, 2 * lanes), BF16),
            jax.ShapeDtypeStruct((2 * rows, lanes), BF16),
        ],
        in_specs=[SMEM] + [VMEM] * 5,
        out_specs=[VMEM, VMEM],
        scratch_shapes=[
            pltpu.VMEM((lanes // 128, rows, 128), F32),
        ],
        compiler_params=params(14),
        cost_estimate=pl.CostEstimate(
            flops=2 * 2 * rows * width * 3 * lanes,
            bytes_accessed=2 * width * (2 * rows + 3 * lanes),
            transcendentals=0,
        ),
        name="project",
    )(meta, x_own, x_other, w_q, w_k, w_v)


def attend(queries, keys, values, bias):
    rows = queries.shape[0]
    low = lax.broadcasted_iota(jnp.int32, (rows, 128), 1) < HEAD_DIM
    zero = jnp.zeros_like(queries)
    stacked = jnp.concatenate([jnp.where(low, queries, zero), jnp.where(low, zero, queries)], axis=0)
    scores = lax.dot_general(
        stacked, keys, (((1,), (1,)), ((), ())), preferred_element_type=F32
    )
    scores = scores * (HEAD_DIM**-0.5 * LOG2E) + bias
    maxima = jnp.maximum(jnp.max(scores, axis=1, keepdims=True), FLOOR)
    weights = jnp.exp2(scores - maxima)
    totals = jnp.sum(weights, axis=1, keepdims=True)
    summed = jnp.dot(weights.astype(BF16), values, preferred_element_type=F32)
    pick = lambda item: jnp.where(low, item[:rows], item[rows:])
    return pick(summed), pick(maxima), pick(totals)


def merge(first, second):
    o1, m1, l1 = first
    o2, m2, l2 = second
    top = jnp.maximum(m1, m2)
    a, b = jnp.exp2(m1 - top), jnp.exp2(m2 - top)
    return o1 * a + o2 * b, top, l1 * a + l2 * b


def near_distance(keys_before, keys_own):
    tile = FAR_DILATION * SUB
    token = lambda n: FAR_DILATION * (n % SUB) + n // SUB
    shape = (tile, (tile if keys_before else 0) + (tile if keys_own else 0))
    row = token(lax.broadcasted_iota(jnp.int32, shape, 0))
    col = lax.broadcasted_iota(jnp.int32, shape, 1)
    if keys_before:
        key = jnp.where(col < tile, token(col) - tile, token(col - tile))
    else:
        key = token(col)
    return row - key


def middle_distance(keys_before, keys_own, chunks):
    group = FAR_DILATION // MIDDLE_DILATION
    size = chunks * group * SUB
    step = lambda n: (n // (group * SUB)) * (group * SUB) + group * (n % SUB) + (n // SUB) % group
    shape = (size, (size if keys_before else 0) + (size if keys_own else 0))
    row = step(lax.broadcasted_iota(jnp.int32, shape, 0))
    col = lax.broadcasted_iota(jnp.int32, shape, 1)
    if keys_before:
        key = jnp.where(col < size, step(col) - size, step(col - size))
    else:
        key = step(col)
    return row - key


def bias_of(distance, slope, stride):
    allowed = (distance >= 0) & (distance <= WINDOW_KEY_STEPS)
    return jnp.where(allowed, distance.astype(F32) * (slope * (-float(stride))), MASKED)


def rows_of(ref, starts, lanes):
    return jnp.concatenate([ref[pl.ds(aligned(s, SUB), SUB), lanes] for s in starts], axis=0)


def middle_starts(block, residue, chunks):
    tile = FAR_DILATION * SUB
    group = FAR_DILATION // MIDDLE_DILATION
    return [
        (block * chunks + s) * tile + (residue + MIDDLE_DILATION * b) * SUB
        for s in range(chunks)
        for b in range(group)
    ]


def far_starts(residue, chunks):
    return [g * FAR_DILATION * SUB + residue * SUB for g in range(chunks)]


def fold_in(refs, starts, lanes, new):
    size = SUB
    for n, start in enumerate(starts):
        where = (pl.ds(aligned(start, SUB), size), lanes)
        old = tuple(ref[where] for ref in refs)
        piece = tuple(item[n * size : (n + 1) * size] for item in new)
        for ref, value in zip(refs, merge(old, piece)):
            ref[where] = value


def pair_lanes(pair, offset=0):
    return slice(offset + pair * 128, offset + (pair + 1) * 128)


def local_kernel(meta, slopes, q_mine, q_part, kv_mine, kv_part, o_ref, m_ref, l_ref, q, kv, near, mid):
    y = meta[2]
    block, lanes = q_mine.shape
    pairs = lanes // 128
    tile = FAR_DILATION * SUB
    chunks = block // tile
    mine = pl.ds(aligned(y * block, block), block)
    part = pl.ds(aligned((1 - y) * block, block), block)
    q[mine], q[part] = q_mine[...], q_part[...]
    kv[mine], kv[part] = kv_mine[...], kv_part[...]
    distance = near_distance(True, True)
    for head in range(2 * pairs):
        near[head] = bias_of(distance, slopes[head], 1)
    distance = middle_distance(True, True, chunks)
    for head in range(2 * pairs):
        mid[head] = bias_of(distance, slopes[head], MIDDLE_DILATION)
    refs = (o_ref, m_ref, l_ref)
    step = 64
    per_tile = tile // step

    def near_step(tile_index, inner, before):
        start = aligned(tile_index * tile + inner * step, step)
        first = aligned((tile_index - 1) * tile if before else tile_index * tile, tile)
        count = 2 * tile if before else tile
        for pair in range(pairs):
            select = pl.ds(aligned(inner * step, step), step)
            columns = slice(0, 2 * tile) if before else slice(tile, 2 * tile)
            bias = jnp.concatenate(
                [near[2 * pair, select, columns], near[2 * pair + 1, select, columns]], axis=0
            )
            result = attend(
                q[pl.ds(start, step), pair_lanes(pair)],
                kv[pl.ds(first, count), pair_lanes(pair)],
                kv[pl.ds(first, count), pair_lanes(pair, lanes)],
                bias,
            )
            for ref, value in zip(refs, result):
                ref[pl.ds(start, step), pair_lanes(pair)] = value

    @pl.loop(0, per_tile)
    def _(n):
        near_step(0, n, False)

    @pl.loop(0, (2 * chunks - 1) * per_tile)
    def _(n):
        near_step(1 + n // per_tile, n % per_tile, True)

    size = mid.shape[1]

    @pl.loop(0, MIDDLE_DILATION)
    def _(residue):
        for index in range(2):
            starts = middle_starts(index, residue, chunks)
            key_starts = (middle_starts(0, residue, chunks) if index else []) + starts
            columns = slice(0, 2 * size) if index else slice(size, 2 * size)
            for pair in range(pairs):
                bias = jnp.concatenate([mid[2 * pair, :, columns], mid[2 * pair + 1, :, columns]], axis=0)
                result = attend(
                    rows_of(q, starts, pair_lanes(pair)),
                    rows_of(kv, key_starts, pair_lanes(pair)),
                    rows_of(kv, key_starts, pair_lanes(pair, lanes)),
                    bias,
                )
                fold_in(refs, starts, pair_lanes(pair), result)


def local_attention(meta, slopes, q_mine, q_part, kv_mine, kv_part):
    block, lanes = q_mine.shape
    tile = FAR_DILATION * SUB
    state = jax.ShapeDtypeStruct((2 * block, lanes), F32)
    heads = lanes // HEAD_DIM
    size = block // MIDDLE_DILATION
    return pl.pallas_call(
        local_kernel,
        out_shape=[state] * 3,
        in_specs=[SMEM, SMEM] + [VMEM] * 4,
        out_specs=[VMEM] * 3,
        scratch_shapes=[
            pltpu.VMEM((2 * block, lanes), BF16),
            pltpu.VMEM((2 * block, 2 * lanes), BF16),
            pltpu.VMEM((heads, tile, 2 * tile), F32),
            pltpu.VMEM((heads, size, 2 * size), F32),
        ],
        compiler_params=params(20),
        cost_estimate=pl.CostEstimate(flops=4 * 10**9, bytes_accessed=4 * 10**6, transcendentals=0),
        name="local",
    )(meta, slopes, q_mine, q_part, kv_mine, kv_part)


def before_kernel(
    meta, slopes, gate, q_mine, q_part, kv_mine, kv_part, kv_a, kv_b, o_in, m_in, l_in,
    o_ref, m_ref, l_ref, q, kv, past, near, mid, far,
):
    y = meta[2]
    block, lanes = q_mine.shape
    pairs = lanes // 128
    tile = FAR_DILATION * SUB
    chunks = block // tile
    mine = pl.ds(aligned(y * block, block), block)
    part = pl.ds(aligned((1 - y) * block, block), block)
    q[mine], q[part] = q_mine[...], q_part[...]
    kv[mine], kv[part] = kv_mine[...], kv_part[...]
    past[mine], past[part] = kv_a[...], kv_b[...]
    o_ref[...], m_ref[...], l_ref[...] = o_in[...], m_in[...], l_in[...]
    closed = gate[0]
    size = mid.shape[1]
    row = lax.broadcasted_iota(jnp.int32, far.shape[1:], 0)
    col = lax.broadcasted_iota(jnp.int32, far.shape[1:], 1)
    half = far.shape[2] // 2
    steps = row - col + half
    for head in range(2 * pairs):
        far[head] = bias_of(steps, slopes[head], FAR_DILATION) + jnp.where(col < half, closed, 0.0)
        near[head] = bias_of(near_distance(True, False), slopes[head], 1) + closed
        mid[head] = bias_of(middle_distance(True, False, chunks), slopes[head], MIDDLE_DILATION) + closed
    refs = (o_ref, m_ref, l_ref)

    for residue in range(FAR_DILATION):
        starts = far_starts(residue, 2 * chunks)
        for pair in range(pairs):
            keys = [rows_of(ref, starts, pair_lanes(pair)) for ref in (past, kv)]
            values = [rows_of(ref, starts, pair_lanes(pair, lanes)) for ref in (past, kv)]
            result = attend(
                rows_of(q, starts, pair_lanes(pair)),
                jnp.concatenate(keys, axis=0),
                jnp.concatenate(values, axis=0),
                jnp.concatenate([far[2 * pair], far[2 * pair + 1]], axis=0),
            )
            fold_in(refs, starts, pair_lanes(pair), result)

    step = 64
    last = (2 * chunks - 1) * tile

    @pl.loop(0, tile // step)
    def _(n):
        select = pl.ds(aligned(n * step, step), step)
        for pair in range(pairs):
            result = attend(
                q[select, pair_lanes(pair)],
                past[last : last + tile, pair_lanes(pair)],
                past[last : last + tile, pair_lanes(pair, lanes)],
                jnp.concatenate([near[2 * pair, select], near[2 * pair + 1, select]], axis=0),
            )
            old = tuple(ref[select, pair_lanes(pair)] for ref in refs)
            for ref, value in zip(refs, merge(old, result)):
                ref[select, pair_lanes(pair)] = value

    @pl.loop(0, MIDDLE_DILATION)
    def _(residue):
        starts = middle_starts(0, residue, chunks)
        key_starts = middle_starts(1, residue, chunks)
        for pair in range(pairs):
            result = attend(
                rows_of(q, starts, pair_lanes(pair)),
                rows_of(past, key_starts, pair_lanes(pair)),
                rows_of(past, key_starts, pair_lanes(pair, lanes)),
                jnp.concatenate([mid[2 * pair], mid[2 * pair + 1]], axis=0),
            )
            fold_in(refs, starts, pair_lanes(pair), result)


def before_attention(meta, slopes, gate, q_mine, q_part, kv_mine, kv_part, kv_a, kv_b, state):
    block, lanes = q_mine.shape
    tile = FAR_DILATION * SUB
    shape = jax.ShapeDtypeStruct((2 * block, lanes), F32)
    heads = lanes // HEAD_DIM
    size = block // MIDDLE_DILATION
    reach = 2 * block // FAR_DILATION
    return pl.pallas_call(
        before_kernel,
        out_shape=[shape] * 3,
        in_specs=[SMEM, SMEM, SMEM] + [VMEM] * 9,
        out_specs=[VMEM] * 3,
        scratch_shapes=[
            pltpu.VMEM((2 * block, lanes), BF16),
            pltpu.VMEM((2 * block, 2 * lanes), BF16),
            pltpu.VMEM((2 * block, 2 * lanes), BF16),
            pltpu.VMEM((heads, tile, tile), F32),
            pltpu.VMEM((heads, size, size), F32),
            pltpu.VMEM((heads, reach, 2 * reach), F32),
        ],
        compiler_params=params(24),
        cost_estimate=pl.CostEstimate(flops=2 * 10**9, bytes_accessed=4 * 10**6, transcendentals=0),
        name="before",
    )(meta, slopes, gate, q_mine, q_part, kv_mine, kv_part, kv_a, kv_b, *state)


def selector(lanes, part):
    shape = (16, lanes)
    row = lax.broadcasted_iota(jnp.int32, shape, 0)
    lane = lax.broadcasted_iota(jnp.int32, shape, 1)
    heads = lanes // HEAD_DIM
    return jnp.where((row // heads == part) & (lane == (row % heads) * HEAD_DIM), 1.0, 0.0).astype(BF16)


def spreader(lanes):
    shape = (16, lanes)
    row = lax.broadcasted_iota(jnp.int32, shape, 0)
    lane = lax.broadcasted_iota(jnp.int32, shape, 1)
    heads = lanes // HEAD_DIM
    return jnp.where((row < 3 * heads) & (lane // HEAD_DIM == row % heads), 1.0, 0.0).astype(BF16)


def pack_sums(sums):
    lanes = sums.shape[1]
    total = jnp.zeros((16, sums.shape[0]), F32)
    for part in range(3):
        piece = sums.astype(BF16)
        sums = sums - piece.astype(F32)
        total = total + lax.dot_general(
            selector(lanes, part), piece, (((1,), (1,)), ((), ())), preferred_element_type=F32
        )
    return total.astype(BF16)


def unpack_sums(packed, lanes):
    return lax.dot_general(packed, spreader(lanes), (((0,), (0,)), ((), ())), preferred_element_type=F32)


def remote_kernel(meta, slopes, gate, after, q_a, q_b, kv_a, kv_b, own_ref, other_ref, q, kv, far, out, sums):
    y = meta[2]
    block, lanes = q_a.shape
    pairs = lanes // 128
    tile = FAR_DILATION * SUB
    chunks = block // tile
    mine = pl.ds(aligned(y * block, block), block)
    part = pl.ds(aligned((1 - y) * block, block), block)
    q[mine], q[part] = q_a[...], q_b[...]
    kv[mine], kv[part] = kv_a[...], kv_b[...]
    closed = gate[0]
    row = lax.broadcasted_iota(jnp.int32, far.shape[1:], 0)
    col = lax.broadcasted_iota(jnp.int32, far.shape[1:], 1)
    steps = row - col + 2 * far.shape[2]
    for head in range(2 * pairs):
        far[head] = bias_of(steps, slopes[head], FAR_DILATION) + closed

    for residue in range(FAR_DILATION):
        starts = far_starts(residue, 2 * chunks)
        for pair in range(pairs):
            o, m, l = attend(
                rows_of(q, starts, pair_lanes(pair)),
                rows_of(kv, starts, pair_lanes(pair)),
                rows_of(kv, starts, pair_lanes(pair, lanes)),
                jnp.concatenate([far[2 * pair], far[2 * pair + 1]], axis=0),
            )
            some = l > 0.0
            safe = jnp.where(some, l, 1.0)
            o = o / safe
            s = jnp.where(some, m + jnp.log2(safe), FLOOR)
            for n, start in enumerate(starts):
                where = (pl.ds(aligned(start, SUB), SUB), pair_lanes(pair))
                out[where] = o[n * SUB : (n + 1) * SUB].astype(BF16)
                sums[where] = s[n * SUB : (n + 1) * SUB]

    for select, ref in ((mine, own_ref), (part, other_ref)):
        ref[:block] = out[select]
        packed = pack_sums(sums[select])
        for n in range(block // lanes):
            ref[block + 16 * n : block + 16 * (n + 1)] = packed[:, n * lanes : (n + 1) * lanes]


def remote_attention(meta, slopes, gate, after, q_a, q_b, kv_a, kv_b):
    block, lanes = q_a.shape
    heads = lanes // HEAD_DIM
    reach = 2 * block // FAR_DILATION
    shape = jax.ShapeDtypeStruct((block + 16 * (block // lanes), lanes), BF16)
    return pl.pallas_call(
        remote_kernel,
        out_shape=[shape] * 2,
        in_specs=[SMEM, SMEM, SMEM, ANY] + [VMEM] * 4,
        out_specs=[VMEM] * 2,
        scratch_shapes=[
            pltpu.VMEM((2 * block, lanes), BF16),
            pltpu.VMEM((2 * block, 2 * lanes), BF16),
            pltpu.VMEM((heads, reach, reach), F32),
            pltpu.VMEM((2 * block, lanes), BF16),
            pltpu.VMEM((2 * block, lanes), F32),
        ],
        compiler_params=params(12),
        cost_estimate=pl.CostEstimate(flops=10**9, bytes_accessed=2 * 10**6, transcendentals=0),
        name="remote",
    )(meta, slopes, gate, after, q_a, q_b, kv_a, kv_b)


def finish_kernel(meta, gate, o_in, m_in, l_in, far_in, stay_ref, go_ref, o_s, m_s, l_s, turned):
    which, tp = meta[0], meta[1]
    block, lanes = o_s.shape
    tile = FAR_DILATION * SUB
    chunks = block // tile
    select = pl.ds(aligned(which * block, block), block)
    o_s[...], m_s[...], l_s[...] = o_in[select], m_in[select], l_in[select]
    per = lanes // tile
    for s in range(chunks):
        rows = slice(s * tile, (s + 1) * tile)
        packed = far_in[block + 16 * (s // per) : block + 16 * (s // per) + 16, (s % per) * tile : (s % per + 1) * tile]
        far_sums = unpack_sums(packed, lanes) + gate[0]
        o, m, l = merge(
            (o_s[rows], m_s[rows], l_s[rows]),
            (far_in[rows].astype(F32), far_sums, jnp.ones_like(far_sums)),
        )
        o_s[rows] = o / l
        m_s[rows] = (m + jnp.log2(l)) * LN2
    for item, ref in enumerate((o_s, m_s)):
        for s in range(chunks):
            for residue in range(FAR_DILATION):
                for part in range(lanes // 128):
                    turned[item, part, pl.ds(s * tile + residue, SUB, stride=FAR_DILATION), :] = ref[
                        s * tile + residue * SUB : s * tile + (residue + 1) * SUB, part * 128 : (part + 1) * 128
                    ]
    half = block // 2
    for part in range(lanes // 128):
        for ref, place in ((stay_ref, tp * half), (go_ref, (1 - tp) * half)):
            ref[:half, part * 128 : (part + 1) * 128] = turned[0, part, pl.ds(aligned(place, half), half), :].astype(BF16)
    sums = jnp.concatenate([turned[1, part] for part in range(lanes // 128)], axis=1)
    packed = pack_sums(sums)
    for n in range(block // lanes):
        stay_ref[half + 16 * n : half + 16 * (n + 1)] = packed[:, n * lanes : (n + 1) * lanes]


def finish(meta, gate, state, far):
    lanes = far.shape[1]
    block = state[0].shape[0] // 2
    half = block // 2
    return pl.pallas_call(
        finish_kernel,
        out_shape=[
            jax.ShapeDtypeStruct((half + 16 * (block // lanes), lanes), BF16),
            jax.ShapeDtypeStruct((half, lanes), BF16),
        ],
        in_specs=[SMEM, SMEM] + [VMEM] * 4,
        out_specs=[VMEM] * 2,
        scratch_shapes=[
            pltpu.VMEM((block, lanes), F32),
            pltpu.VMEM((block, lanes), F32),
            pltpu.VMEM((block, lanes), F32),
            pltpu.VMEM((2, lanes // 128, block, 128), F32),
        ],
        compiler_params=params(14),
        cost_estimate=pl.CostEstimate(flops=5 * 10**8, bytes_accessed=2 * 10**6, transcendentals=0),
        name="finish",
    )(meta, gate, *state, far)


def output_kernel(meta, stay, same, tp_piece, cross, w_mine, w_other, out_ref, sums_ref):
    y = meta[2]
    half, width = out_ref.shape
    lanes = stay.shape[1]
    heads = lanes // HEAD_DIM
    block = 2 * half
    near_rows = pl.ds(aligned(y * lanes, lanes), lanes)
    far_rows = pl.ds(aligned((1 - y) * lanes, lanes), lanes)
    step = 512
    for start in range(0, width, step):
        columns = slice(start, start + step)
        first = jnp.dot(stay[:half], w_mine[near_rows, columns], preferred_element_type=F32)
        first += jnp.dot(same[:half], w_mine[far_rows, columns], preferred_element_type=F32)
        second = jnp.dot(tp_piece[...], w_other[near_rows, columns], preferred_element_type=F32)
        second += jnp.dot(cross[...], w_other[far_rows, columns], preferred_element_type=F32)
        out_ref[:, columns] = (first.astype(BF16).astype(F32) + second.astype(BF16).astype(F32)).astype(BF16)
    halves = []
    for ref in (stay, same):
        both = []
        for n in range(block // lanes):
            packed = ref[half + 16 * n : half + 16 * (n + 1)].astype(F32)
            total = packed[:heads] + packed[heads : 2 * heads] + packed[2 * heads : 3 * heads]
            both.append(total)
        halves.append(jnp.concatenate(both, axis=1))
    low = jnp.where(y == 0, halves[0], halves[1])
    high = jnp.where(y == 0, halves[1], halves[0])
    sums_ref[...] = jnp.concatenate([low, high], axis=0)


def output(meta, stay, same, tp_piece, cross, w_mine, w_other):
    half, lanes = tp_piece.shape
    width = w_mine.shape[1]
    heads = lanes // HEAD_DIM
    return pl.pallas_call(
        output_kernel,
        out_shape=[
            jax.ShapeDtypeStruct((half, width), BF16),
            jax.ShapeDtypeStruct((2 * heads, 2 * half), F32),
        ],
        in_specs=[SMEM] + [VMEM] * 6,
        out_specs=[VMEM] * 2,
        compiler_params=params(16),
        cost_estimate=pl.CostEstimate(
            flops=2 * half * width * 4 * lanes, bytes_accessed=6 * 10**6, transcendentals=0
        ),
        name="output",
    )(meta, stay, same, tp_piece, cross, w_mine, w_other)


def body(tokens, w_query, w_key, w_value, w_out):
    half, _ = tokens.shape
    block = 2 * half
    width = w_query.shape[1]
    lanes = width // 2
    count = lax.axis_size("sp")
    pair = 2
    assert lax.axis_size("tp") == 2 and count % pair == 0
    assert REACH == 2 * pair * block and half == FAR_DILATION * SUB and lanes % 128 == 0
    ahead = [(n, n + pair) for n in range(count - pair)]
    back = [(n + pair, n) for n in range(count - pair)]
    beside = [(n, n ^ 1) for n in range(count)]
    swap = [(0, 1), (1, 0)]
    crossed = [(2 * n + c, 2 * (n ^ 1) + 1 - c) for n in range(count) for c in range(2)]

    place = lax.axis_index("sp")
    y = place % 2
    z = place // 2
    tp = lax.axis_index("tp")
    meta_mine = jnp.stack([y, tp, y]).astype(jnp.int32)
    meta_other = jnp.stack([1 - y, tp, y]).astype(jnp.int32)
    heads = lanes // HEAD_DIM
    head_ids = tp * (2 * heads) + y * heads + jnp.arange(1, heads + 1, dtype=jnp.int32)
    slopes = jnp.exp2(-ALIBI_EXP * head_ids.astype(F32) / HEADS) * LOG2E
    gate = jnp.where(z > 0, 0.0, MASKED).astype(F32).reshape(1)

    x_other = lax.ppermute(tokens, "tp", swap)
    kv_t, q_t = project(meta_other, tokens, x_other, w_query, w_key, w_value, lanes)
    kv_m, q_m = project(meta_mine, tokens, x_other, w_query, w_key, w_value, lanes)
    kv_p = lax.ppermute(kv_t, "sp", beside)
    kv_a = lax.ppermute(kv_m, "sp", ahead)
    q_p = lax.ppermute(q_t, "sp", beside)
    q_a = lax.ppermute(q_m, "sp", back)
    kv_b = lax.ppermute(kv_p, "sp", ahead)
    q_b = lax.ppermute(q_p, "sp", back)
    w_other = lax.ppermute(w_out, "tp", swap)
    state = local_attention(meta_mine, slopes, q_m, q_p, kv_m, kv_p)
    far_own, far_other = remote_attention(meta_mine, slopes, gate, state[2], q_a, q_b, kv_a, kv_b)
    far_p = lax.ppermute(far_other, "sp", ahead)
    far_m = lax.ppermute(far_own, "sp", ahead)
    state = before_attention(meta_mine, slopes, gate, q_m, q_p, kv_m, kv_p, kv_a, kv_b, state)
    same_go, cross_go = finish(meta_other, gate, state, far_p)
    same = lax.ppermute(same_go, "sp", beside)
    cross = lax.ppermute(cross_go, ("sp", "tp"), crossed)
    stay, tp_go = finish(meta_mine, gate, state, far_m)
    tp_piece = lax.ppermute(tp_go, "tp", swap)
    mixed, sums = output(meta_mine, stay, same, tp_piece, cross, w_out, w_other)
    return mixed, sums


def solution(mesh):
    in_specs = (
        P(("grp", "sp", "tp"), None),
        P(None, "tp"),
        P(None, "tp"),
        P(None, "tp"),
        P("tp", None),
    )
    out_specs = (P(("grp", "sp", "tp"), None), P("tp", ("grp", "sp")))
    return jax.shard_map(body, mesh=mesh, in_specs=in_specs, out_specs=out_specs, check_vma=False)
```

```python
import functools
import math

import jax
import jax.numpy as jnp
from jax import lax
from jax.experimental import pallas as pl
from jax.experimental.pallas import tpu as pltpu
from jax.sharding import PartitionSpec as P


HEADS = 16
HEAD_DIM = 64
WINDOW_KEY_STEPS = 128
MIDDLE_DILATION = 4
FAR_DILATION = 16
REACH = 2048
ALIBI_EXP = 16.0

LOG2E = math.log2(math.e)
LN2 = math.log(2.0)
MASKED = -1e30
FLOOR = -1e25
F32 = jnp.float32
BF16 = jnp.bfloat16
ANY = pl.BlockSpec(memory_space=pl.ANY)
VMEM = pl.BlockSpec(memory_space=pltpu.VMEM)
MIB = 1024 * 1024


def params(limit):
    return pltpu.CompilerParams(vmem_limit_bytes=limit * MIB)


SUB = 16


def aligned(value, multiple):
    return value if isinstance(value, int) else pl.multiple_of(value, multiple)


def places():
    place = lax.axis_index("sp")
    return place % 2, place // 2, lax.axis_index("tp")


def call(kernel, results, inputs, scratch=(), limit=12, flops=10**9, loose=0):
    return pl.pallas_call(
        kernel,
        out_shape=[jax.ShapeDtypeStruct(shape, kind) for shape, kind in results],
        in_specs=[VMEM] * (len(inputs) - loose) + [ANY] * loose,
        out_specs=[VMEM] * len(results),
        scratch_shapes=list(scratch),
        compiler_params=params(limit),
        cost_estimate=pl.CostEstimate(flops=flops, bytes_accessed=10**6, transcendentals=0),
    )(*inputs)


def project_kernel(first, weights, *refs):
    x_own, x_other = refs[:2]
    ws = refs[2 : 2 + weights]
    outs, acc = refs[2 + weights : -1], refs[-1]
    y, _, tp = places()
    rows = x_own.shape[0]
    slot = 0
    for w in ws:
        for start in first:
            for half, x in enumerate((x_own, x_other)):
                result = jnp.dot(x[...], w[:, start : start + 256], preferred_element_type=F32)
                acc[slot, 0], acc[slot, 1] = result[:, :128], result[:, 128:]
                place = (tp if half == 0 else 1 - tp) * rows
                index = slot // 2 if len(first) > 1 or weights > 1 else 0
                for side, out in enumerate(outs):
                    source = 1 - y if side == 0 else y
                    for residue in range(FAR_DILATION):
                        chunk = acc[slot, source, pl.ds(residue, SUB, stride=FAR_DILATION), :].astype(BF16)
                        where = pl.ds(aligned(place + residue * SUB, SUB), SUB)
                        out[where, index * 128 : (index + 1) * 128] = chunk
                slot += 1


def project(x_own, x_other, weights, first):
    rows, width = x_own.shape
    shape = ((2 * rows, 256), BF16)
    slots = 2 * len(first) * len(weights)
    return call(
        functools.partial(project_kernel, first, len(weights)),
        [shape, shape],
        [x_own, x_other, *weights],
        [pltpu.VMEM((slots, 2, rows, 128), F32)],
        limit=10,
        flops=2 * slots * rows * width * 256,
    )


def attend(queries, keys, values, bias):
    rows = queries.shape[0]
    low = lax.broadcasted_iota(jnp.int32, (rows, 128), 1) < HEAD_DIM
    zero = jnp.zeros_like(queries)
    stacked = jnp.concatenate([jnp.where(low, queries, zero), jnp.where(low, zero, queries)], axis=0)
    scores = lax.dot_general(
        stacked, keys, (((1,), (1,)), ((), ())), preferred_element_type=F32
    )
    scores = scores * (HEAD_DIM**-0.5 * LOG2E) + bias
    maxima = jnp.maximum(jnp.max(scores, axis=1, keepdims=True), FLOOR)
    weights = jnp.exp2(scores - maxima)
    totals = jnp.sum(weights, axis=1, keepdims=True)
    summed = jnp.dot(weights.astype(BF16), values, preferred_element_type=F32)
    pick = lambda item: jnp.where(low, item[:rows], item[rows:])
    return pick(summed), pick(maxima), pick(totals)


def merge(first, second):
    o1, m1, l1 = first
    o2, m2, l2 = second
    top = jnp.maximum(m1, m2)
    a, b = jnp.exp2(m1 - top), jnp.exp2(m2 - top)
    return o1 * a + o2 * b, top, l1 * a + l2 * b


def near_distance(keys_before, keys_own):
    tile = FAR_DILATION * SUB
    token = lambda n: FAR_DILATION * (n % SUB) + n // SUB
    shape = (tile, (tile if keys_before else 0) + (tile if keys_own else 0))
    row = token(lax.broadcasted_iota(jnp.int32, shape, 0))
    col = lax.broadcasted_iota(jnp.int32, shape, 1)
    if keys_before:
        key = jnp.where(col < tile, token(col) - tile, token(col - tile))
    else:
        key = token(col)
    return row - key


def middle_distance(keys_before, keys_own, chunks):
    group = FAR_DILATION // MIDDLE_DILATION
    size = chunks * group * SUB
    step = lambda n: (n // (group * SUB)) * (group * SUB) + group * (n % SUB) + (n // SUB) % group
    shape = (size, (size if keys_before else 0) + (size if keys_own else 0))
    row = step(lax.broadcasted_iota(jnp.int32, shape, 0))
    col = lax.broadcasted_iota(jnp.int32, shape, 1)
    if keys_before:
        key = jnp.where(col < size, step(col) - size, step(col - size))
    else:
        key = step(col)
    return row - key


def bias_of(distance, slope, stride):
    allowed = (distance >= 0) & (distance <= WINDOW_KEY_STEPS)
    return jnp.where(allowed, distance.astype(F32) * (slope * (-float(stride))), MASKED)


def rows_of(ref, starts, lanes):
    return jnp.concatenate([ref[pl.ds(aligned(s, SUB), SUB), lanes] for s in starts], axis=0)


def middle_starts(block, residue, chunks):
    tile = FAR_DILATION * SUB
    group = FAR_DILATION // MIDDLE_DILATION
    return [
        (block * chunks + s) * tile + (residue + MIDDLE_DILATION * b) * SUB
        for s in range(chunks)
        for b in range(group)
    ]


def far_starts(residue, chunks):
    return [g * FAR_DILATION * SUB + residue * SUB for g in range(chunks)]


def fold_in(refs, starts, lanes, new):
    size = SUB
    for n, start in enumerate(starts):
        where = (pl.ds(aligned(start, SUB), size), lanes)
        old = tuple(ref[where] for ref in refs)
        piece = tuple(item[n * size : (n + 1) * size] for item in new)
        for ref, value in zip(refs, merge(old, piece)):
            ref[where] = value


def pair_lanes(pair, offset=0):
    return slice(offset + pair * 128, offset + (pair + 1) * 128)


def bias_kernel(near, mid, far):
    heads = near.shape[0]
    y, _, tp = places()
    tile = FAR_DILATION * SUB
    chunks = mid.shape[1] // (tile // MIDDLE_DILATION)
    near_steps = near_distance(True, True)
    mid_steps = middle_distance(True, True, chunks)
    row = lax.broadcasted_iota(jnp.int32, far.shape[2:], 0)
    col = lax.broadcasted_iota(jnp.int32, far.shape[2:], 1)
    far_slope = lambda head, shape: jnp.exp2(
        jnp.full(shape, -ALIBI_EXP / HEADS, F32)
        * (tp * 2 * heads + (head // 2) * 4 + y * 2 + head % 2 + 1).astype(F32)
    ) * LOG2E
    for head in range(heads):
        slope = far_slope(head, (1, 1))
        near[head] = bias_of(near_steps, slope, 1)
        mid[head] = bias_of(mid_steps, slope, MIDDLE_DILATION)
        for back in range(3):
            far[back, head] = bias_of(row - col + back * far.shape[3], slope, FAR_DILATION)


def biases(block, heads):
    tile = FAR_DILATION * SUB
    size = block // MIDDLE_DILATION
    reach = 2 * block // FAR_DILATION
    return call(
        bias_kernel,
        [((heads, tile, 2 * tile), F32), ((heads, size, 2 * size), F32), ((3, heads, reach, reach), F32)],
        [],
        limit=8,
        flops=10**9,
        loose=0,
    )


def stacked(ref, pair, rows, columns, extra=None):
    both = jnp.concatenate([ref[2 * pair, rows, columns], ref[2 * pair + 1, rows, columns]], axis=0)
    return both if extra is None else both + extra


def closed_gate():
    _, z, _ = places()
    return jnp.where(z > 0, 0.0, MASKED).astype(F32)


def place_pair(target, mine, part):
    y, _, _ = places()
    block = mine.shape[0]
    target[pl.ds(aligned(y * block, block), block)] = mine[...]
    target[pl.ds(aligned((1 - y) * block, block), block)] = part[...]


KEYS, VALUES = slice(0, 128), slice(128, 256)


def block_kernel(near, mid, q, kv0, kv1, *rest):
    o_ref, m_ref, l_ref = rest[-3:]
    block = q.shape[0]
    tile = FAR_DILATION * SUB
    chunks = block // tile
    refs = (o_ref, m_ref, l_ref)
    step = 64
    size = mid.shape[1]
    for pair, kv in enumerate((kv0, kv1)):
        for index in range(chunks):
            first = max(index - 1, 0) * tile
            width = tile if index == 0 else 2 * tile
            columns = slice(2 * tile - width, 2 * tile)
            for inner in range(tile // step):
                start = index * tile + inner * step
                result = attend(
                    q[start : start + step, pair_lanes(pair)],
                    kv[first : first + width, KEYS],
                    kv[first : first + width, VALUES],
                    stacked(near, pair, slice(inner * step, (inner + 1) * step), columns),
                )
                for ref, value in zip(refs, result):
                    ref[start : start + step, pair_lanes(pair)] = value
        for residue in range(MIDDLE_DILATION):
            starts = middle_starts(0, residue, chunks)
            result = attend(
                rows_of(q, starts, pair_lanes(pair)),
                rows_of(kv, starts, KEYS),
                rows_of(kv, starts, VALUES),
                stacked(mid, pair, slice(0, size), slice(size, 2 * size)),
            )
            fold_in(refs, starts, pair_lanes(pair), result)


def block_attention(bias, q, kv0, kv1, after=()):
    return call(
        block_kernel,
        [(q.shape, F32)] * 3,
        [bias[0], bias[1], q, kv0, kv1, *after],
        limit=10,
        flops=4 * 10**9,
        loose=len(after),
    )


def windows(refs, q, kvs, near, mid, far, before, closed):
    block = q.shape[0] // 2
    tile = FAR_DILATION * SUB
    chunks = block // tile
    back = 1 if before else 0
    query_tile = 0 if before else chunks
    key_tile = (2 * chunks - 1 if before else chunks - 1) * tile
    step = 64
    size = mid.shape[1]
    for pair in range(len(kvs)):
        kv = kvs[pair]
        for residue in range(FAR_DILATION):
            starts = far_starts(residue, 2 * chunks)
            result = attend(
                rows_of(q, starts, pair_lanes(pair)),
                rows_of(kv, starts, KEYS),
                rows_of(kv, starts, VALUES),
                jnp.concatenate([far[back, 2 * pair], far[back, 2 * pair + 1]], axis=0) + closed,
            )
            fold_in(refs, starts, pair_lanes(pair), result)
        for inner in range(tile // step):
            start = query_tile * tile + inner * step
            result = attend(
                q[start : start + step, pair_lanes(pair)],
                kv[key_tile : key_tile + tile, KEYS],
                kv[key_tile : key_tile + tile, VALUES],
                stacked(near, pair, slice(inner * step, (inner + 1) * step), slice(0, tile), closed),
            )
            where = (slice(start, start + step), pair_lanes(pair))
            old = tuple(ref[where] for ref in refs)
            for ref, value in zip(refs, merge(old, result)):
                ref[where] = value
        for residue in range(MIDDLE_DILATION):
            starts = middle_starts(0 if before else 1, residue, chunks)
            key_starts = middle_starts(1 if before else 0, residue, chunks)
            result = attend(
                rows_of(q, starts, pair_lanes(pair)),
                rows_of(kv, key_starts, KEYS),
                rows_of(kv, key_starts, VALUES),
                stacked(mid, pair, slice(0, size), slice(0, size), closed),
            )
            fold_in(refs, starts, pair_lanes(pair), result)


def pair_kernel(near, mid, far, q_mine, q_part, *rest):
    kv_mine, kv_part, mine, part = rest[:2], rest[2:4], rest[4:7], rest[7:10]
    *refs, q_ref, kv = rest[-5:]
    place_pair(q_ref, q_mine, q_part)
    for n in range(2):
        place_pair(kv.at[n], kv_mine[n], kv_part[n])
    for ref, first, second in zip(refs, mine, part):
        place_pair(ref, first, second)
    windows(refs, q_ref, [kv.at[0], kv.at[1]], near, mid, far, False, 0.0)


def pair_attention(bias, q_mine, q_part, kv_mine, kv_part, mine, part, after=()):
    block, lanes = q_mine.shape
    return call(
        pair_kernel,
        [((2 * block, lanes), F32)] * 3 + [((2 * block, lanes), BF16)],
        [*bias, q_mine, q_part, *kv_mine, *kv_part, *mine, *part, *after],
        [pltpu.VMEM((2, 2 * block, 256), BF16)],
        limit=16,
        flops=4 * 10**9,
        loose=len(after),
    )


def before_kernel(near, mid, far, q, kv_a0, kv_b0, kv_a1, kv_b1, o_in, m_in, l_in, *rest):
    o_ref, m_ref, l_ref, past = rest[-4:]
    place_pair(past.at[0], kv_a0, kv_b0)
    place_pair(past.at[1], kv_a1, kv_b1)
    o_ref[...], m_ref[...], l_ref[...] = o_in[...], m_in[...], l_in[...]
    windows((o_ref, m_ref, l_ref), q, [past.at[0], past.at[1]], near, mid, far, True, closed_gate())


def before_attention(bias, q, past, state, after=()):
    return call(
        before_kernel,
        [(q.shape, F32)] * 3,
        [*bias, q, *past, *state, *after],
        [pltpu.VMEM((2, q.shape[0], 256), BF16)],
        limit=16,
        flops=4 * 10**9,
        loose=len(after),
    )


def part_row(shape, block):
    row = lax.broadcasted_iota(jnp.int32, shape, 0) - 8 * block
    lane = lax.broadcasted_iota(jnp.int32, shape, 1)
    return row, lane


def pack_sums(blocks):
    total = 0.0
    for n, sums in enumerate(blocks):
        row, lane = part_row((16, 128), n)
        for part in range(3):
            piece = sums.astype(BF16)
            sums = sums - piece.astype(F32)
            pick = (row // 2 == part) & (row >= 0) & (lane == (row % 2) * HEAD_DIM)
            total = total + lax.dot_general(
                jnp.where(pick, 1.0, 0.0).astype(BF16), piece, (((1,), (1,)), ((), ())), preferred_element_type=F32
            )
    return total.astype(BF16)


def unpack_sums(packed, block):
    row, lane = part_row((16, 128), block)
    pick = (row >= 0) & (row < 6) & (lane // HEAD_DIM == row % 2)
    return lax.dot_general(
        packed, jnp.where(pick, 1.0, 0.0).astype(BF16), (((0,), (0,)), ((), ())), preferred_element_type=F32
    )


def store_packed(ref, first, packed):
    for n in range(packed.shape[1] // 128):
        ref[first + 16 * n : first + 16 * (n + 1)] = packed[:, n * 128 : (n + 1) * 128]


def load_packed(ref, first, count):
    return jnp.concatenate([ref[first + 16 * n : first + 16 * (n + 1)] for n in range(count)], axis=1)


def remote_kernel(pair, far, q_a, q_b, kv_a, kv_b, *rest):
    out_ref, q, kv, sums = rest[-4:]
    block = q_a.shape[0]
    tile = FAR_DILATION * SUB
    chunks = block // tile
    place_pair(q, q_a.at[:, pair_lanes(pair)], q_b.at[:, pair_lanes(pair)])
    place_pair(kv, kv_a, kv_b)
    closed = closed_gate()
    bias = jnp.concatenate([far[2, 2 * pair], far[2, 2 * pair + 1]], axis=0) + closed
    for residue in range(FAR_DILATION):
        starts = far_starts(residue, 2 * chunks)
        o, m, l = attend(rows_of(q, starts, KEYS), rows_of(kv, starts, KEYS), rows_of(kv, starts, VALUES), bias)
        some = l > 0.0
        safe = jnp.where(some, l, 1.0)
        o = o / safe
        s = jnp.where(some, m + jnp.log2(safe), FLOOR)
        for n, start in enumerate(starts):
            where = pl.ds(start, SUB)
            out_ref[where] = o[n * SUB : (n + 1) * SUB].astype(BF16)
            sums[where] = s[n * SUB : (n + 1) * SUB]
    store_packed(out_ref, 2 * block, pack_sums([sums[:block], sums[block:]]))


def remote_attention(pair, far, q_a, q_b, kv_a, kv_b, after=()):
    block = q_a.shape[0]
    return call(
        functools.partial(remote_kernel, pair),
        [((2 * block + 16 * (block // 128), 128), BF16)],
        [far, q_a, q_b, kv_a, kv_b, *after],
        [pltpu.VMEM((2 * block, 128), BF16), pltpu.VMEM((2 * block, 256), BF16), pltpu.VMEM((2 * block, 128), F32)],
        limit=8,
        flops=10**9,
        loose=len(after),
    )[0]


def finish_kernel(pair, o_in, m_in, l_in, far_in, *rest):
    stay_ref, go_ref, same_ref, cross_ref, sums_ref, o_s, turned = rest[-7:]
    y, _, tp = places()
    rows = o_in.shape[0]
    block = rows // 2
    half = block // 2
    tile = FAR_DILATION * SUB
    lanes = pair_lanes(pair)
    closed = closed_gate()
    packed = load_packed(far_in, rows, block // 128)
    for b in range(2):
        far_sums = unpack_sums(packed, b) + closed
        select = slice(b * block, (b + 1) * block)
        o, m, l = merge(
            (o_in[select, lanes], m_in[select, lanes], l_in[select, lanes]),
            (far_in[select].astype(F32), far_sums, jnp.ones_like(far_sums)),
        )
        o_s[0, select] = o / l
        o_s[1, select] = (m + jnp.log2(l)) * LN2
    for item in range(2):
        for s in range(rows // tile):
            for residue in range(FAR_DILATION):
                turned[item, pl.ds(s * tile + residue, SUB, stride=FAR_DILATION), :] = o_s[
                    item, s * tile + residue * SUB : s * tile + (residue + 1) * SUB
                ]
    own, other = y * block, (1 - y) * block
    for ref, start in (
        (stay_ref, own + tp * half),
        (go_ref, own + (1 - tp) * half),
        (same_ref, other + tp * half),
        (cross_ref, other + (1 - tp) * half),
    ):
        ref[:half] = turned[0, pl.ds(aligned(start, half), half), :].astype(BF16)
    sums_ref[...] = pack_sums([turned[1, pl.ds(aligned(own, block), block), :]])
    store_packed(same_ref, half, pack_sums([turned[1, pl.ds(aligned(other, block), block), :]]))


def finish(pair, state, far, after=()):
    rows = state[0].shape[0]
    block, half = rows // 2, rows // 4
    piece = ((half, 128), BF16)
    return call(
        functools.partial(finish_kernel, pair),
        [piece, piece, ((half + 16 * (block // 128), 128), BF16), piece, ((16, block), BF16)],
        [*state, far, *after],
        [pltpu.VMEM((2, rows, 128), F32), pltpu.VMEM((2, rows, 128), F32)],
        limit=8,
        flops=10**9,
        loose=len(after),
    )


def output_kernel(*refs):
    pieces, (w_mine, w_other, out_ref, sums_ref) = (refs[:5], refs[5:10]), refs[10:]
    y, _, _ = places()
    half, width = out_ref.shape
    block = 2 * half
    low = y == 0
    order = lambda mine, part: (jnp.where(low, mine, part), jnp.where(low, part, mine))
    hidden = []
    for first, second in ((0, 1), (2, 3)):
        blocks = []
        for piece in pieces:
            blocks += order(piece[first][:half], piece[second][:half])
        hidden.append(jnp.concatenate(blocks, axis=1))
    step = 512
    for start in range(0, width, step):
        columns = slice(start, start + step)
        first = jnp.dot(hidden[0], w_mine[:, columns], preferred_element_type=F32)
        second = jnp.dot(hidden[1], w_other[:, columns], preferred_element_type=F32)
        out_ref[:, columns] = (first.astype(BF16).astype(F32) + second.astype(BF16).astype(F32)).astype(BF16)
    heads = []
    for piece in pieces:
        sums = []
        for packed in (piece[4][...], load_packed(piece[1], half, block // 128)):
            packed = packed.astype(F32)
            sums.append(packed[0:2] + packed[2:4] + packed[4:6])
        heads += order(*sums)
    sums_ref[...] = jnp.concatenate(heads, axis=0)


def output(pieces, w_mine, w_other):
    half = pieces[0][0].shape[0]
    width = w_mine.shape[1]
    return call(
        output_kernel,
        [((half, width), BF16), ((8, 2 * half), F32)],
        [*pieces[0], *pieces[1], w_mine, w_other],
        limit=12,
        flops=2 * half * width * 1024,
    )


def layer(tokens, w_query, w_key, w_value, w_out):
    half, _ = tokens.shape
    block = 2 * half
    width = w_query.shape[1]
    heads = width // 2 // HEAD_DIM
    count = lax.axis_size("sp")
    assert lax.axis_size("tp") == 2 and count % 2 == 0
    assert REACH == 4 * block and half == FAR_DILATION * SUB and width == 512
    ahead = [(n, (n + 2) % count) for n in range(count)]
    back = [(n + 2, n) for n in range(count - 2)]
    beside = [(n, n ^ 1) for n in range(count)]
    swap = [(0, 1), (1, 0)]
    crossed = [(2 * n + c, 2 * (n ^ 1) + 1 - c) for n in range(count) for c in range(2)]

    x_other = lax.ppermute(tokens, "tp", swap)
    kv_t0, kv_m0 = project(tokens, x_other, [w_key, w_value], [0])
    kv_p0 = lax.ppermute(kv_t0, "sp", beside)
    kv_a0 = lax.ppermute(kv_m0, "sp", ahead)
    q_t, q_m = project(tokens, x_other, [w_query], [0, 256])
    q_p = lax.ppermute(q_t, "sp", beside)
    q_a = lax.ppermute(q_m, "sp", back)
    kv_t1, kv_m1 = project(tokens, x_other, [w_key, w_value], [256])
    kv_p1 = lax.ppermute(kv_t1, "sp", beside)
    kv_a1 = lax.ppermute(kv_m1, "sp", ahead)
    kv_b0 = lax.ppermute(kv_p0, "sp", ahead)
    q_b = lax.ppermute(q_p, "sp", back)
    kv_b1 = lax.ppermute(kv_p1, "sp", ahead)
    w_other = lax.ppermute(w_out, "tp", swap)
    bias = biases(block, heads)
    mine = block_attention(bias, q_m, kv_m0, kv_m1)
    part = block_attention(bias, q_p, kv_p0, kv_p1, mine[:1])
    far0 = remote_attention(0, bias[2], q_a, q_b, kv_a0, kv_b0)
    far_p = lax.ppermute(far0, "sp", ahead)
    *state, q = pair_attention(bias, q_m, q_p, (kv_m0, kv_m1), (kv_p0, kv_p1), mine, part)
    far1 = remote_attention(1, bias[2], q_a, q_b, kv_a1, kv_b1)
    far_m = lax.ppermute(far1, "sp", ahead)
    state = before_attention(bias, q, (kv_a0, kv_b0, kv_a1, kv_b1), state)
    pieces = []
    for pair, far in enumerate((far_p, far_m)):
        stay, go, same, cross, sums = finish(pair, state, far)
        same = lax.ppermute(same, "sp", beside)
        cross = lax.ppermute(cross, ("sp", "tp"), crossed)
        go = lax.ppermute(go, "tp", swap)
        pieces.append((stay, same, go, cross, sums))
    return output(pieces, w_out, w_other)


def solution(mesh):
    in_specs = (
        P(("grp", "sp", "tp"), None),
        P(None, "tp"),
        P(None, "tp"),
        P(None, "tp"),
        P("tp", None),
    )
    out_specs = (P(("grp", "sp", "tp"), None), P("tp", ("grp", "sp")))
    return jax.shard_map(layer, mesh=mesh, in_specs=in_specs, out_specs=out_specs, check_vma=False)
```

```python
import functools
import math

import jax
import jax.numpy as jnp
from jax import lax
from jax.experimental import pallas as pl
from jax.experimental.pallas import tpu as pltpu
from jax.sharding import PartitionSpec as P


HEADS = 16
HEAD_DIM = 64
WINDOW_KEY_STEPS = 128
MIDDLE_DILATION = 4
FAR_DILATION = 16
REACH = 2048
ALIBI_EXP = 16.0

LOG2E = math.log2(math.e)
LN2 = math.log(2.0)
MASKED = -1e30
FLOOR = -1e25
F32 = jnp.float32
BF16 = jnp.bfloat16
ANY = pl.BlockSpec(memory_space=pl.ANY)
VMEM = pl.BlockSpec(memory_space=pltpu.VMEM)

MIB = 1024 * 1024


def params(limit):
    return pltpu.CompilerParams(vmem_limit_bytes=limit * MIB)


SUB = 16


def aligned(value, multiple):
    return value if isinstance(value, int) else pl.multiple_of(value, multiple)


def places():
    place = lax.axis_index("sp")
    return place % 2, place // 2, lax.axis_index("tp")


def call(kernel, results, inputs, scratch=(), limit=12, flops=10**9, loose=0):
    return pl.pallas_call(
        kernel,
        out_shape=[jax.ShapeDtypeStruct(shape, kind) for shape, kind in results],
        in_specs=[VMEM] * (len(inputs) - loose) + [ANY] * loose,
        out_specs=[VMEM] * len(results),
        scratch_shapes=list(scratch),
        compiler_params=params(limit),
        cost_estimate=pl.CostEstimate(flops=flops, bytes_accessed=10**6, transcendentals=0),
    )(*inputs)


def project_kernel(first, weights, *refs):
    x_own, x_other = refs[:2]
    ws = refs[2 : 2 + weights]
    outs, acc = refs[2 + weights : -1], refs[-1]
    y, _, tp = places()
    rows = x_own.shape[0]
    slot = 0
    for w in ws:
        for start in first:
            for half, x in enumerate((x_own, x_other)):
                result = jnp.dot(x[...], w[:, start : start + 256], preferred_element_type=F32)
                acc[slot, 0], acc[slot, 1] = result[:, :128], result[:, 128:]
                place = (tp if half == 0 else 1 - tp) * rows
                index = slot // 2 if len(first) > 1 or weights > 1 else 0
                for side, out in enumerate(outs):
                    source = 1 - y if side == 0 else y
                    for residue in range(FAR_DILATION):
                        chunk = acc[slot, source, pl.ds(residue, SUB, stride=FAR_DILATION), :].astype(BF16)
                        where = pl.ds(aligned(place + residue * SUB, SUB), SUB)
                        out[where, index * 128 : (index + 1) * 128] = chunk
                slot += 1


def project(x_own, x_other, weights, first):
    rows, width = x_own.shape
    shape = ((2 * rows, 256), BF16)
    slots = 2 * len(first) * len(weights)
    return call(
        functools.partial(project_kernel, first, len(weights)),
        [shape, shape],
        [x_own, x_other, *weights],
        [pltpu.VMEM((slots, 2, rows, 128), F32)],
        limit=10,
        flops=2 * slots * rows * width * 256,
    )


def attend(queries, keys, values, bias):
    rows = queries.shape[0]
    low = lax.broadcasted_iota(jnp.int32, (rows, 128), 1) < HEAD_DIM
    zero = jnp.zeros_like(queries)
    stacked = jnp.concatenate([jnp.where(low, queries, zero), jnp.where(low, zero, queries)], axis=0)
    scores = lax.dot_general(
        stacked, keys, (((1,), (1,)), ((), ())), preferred_element_type=F32
    )
    scores = scores * (HEAD_DIM**-0.5 * LOG2E) + bias
    maxima = jnp.maximum(jnp.max(scores, axis=1, keepdims=True), FLOOR)
    weights = jnp.exp2(scores - maxima)
    totals = jnp.sum(weights, axis=1, keepdims=True)
    summed = jnp.dot(weights.astype(BF16), values, preferred_element_type=F32)
    pick = lambda item: jnp.where(low, item[:rows], item[rows:])
    return pick(summed), pick(maxima), pick(totals)


def merge(first, second):
    o1, m1, l1 = first
    o2, m2, l2 = second
    top = jnp.maximum(m1, m2)
    a, b = jnp.exp2(m1 - top), jnp.exp2(m2 - top)
    return o1 * a + o2 * b, top, l1 * a + l2 * b


def near_distance(keys_before, keys_own):
    tile = FAR_DILATION * SUB
    token = lambda n: FAR_DILATION * (n % SUB) + n // SUB
    shape = (tile, (tile if keys_before else 0) + (tile if keys_own else 0))
    row = token(lax.broadcasted_iota(jnp.int32, shape, 0))
    col = lax.broadcasted_iota(jnp.int32, shape, 1)
    if keys_before:
        key = jnp.where(col < tile, token(col) - tile, token(col - tile))
    else:
        key = token(col)
    return row - key


def middle_distance(keys_before, keys_own, chunks):
    group = FAR_DILATION // MIDDLE_DILATION
    size = chunks * group * SUB
    step = lambda n: (n // (group * SUB)) * (group * SUB) + group * (n % SUB) + (n // SUB) % group
    shape = (size, (size if keys_before else 0) + (size if keys_own else 0))
    row = step(lax.broadcasted_iota(jnp.int32, shape, 0))
    col = lax.broadcasted_iota(jnp.int32, shape, 1)
    if keys_before:
        key = jnp.where(col < size, step(col) - size, step(col - size))
    else:
        key = step(col)
    return row - key


def bias_of(distance, slope, stride):
    allowed = (distance >= 0) & (distance <= WINDOW_KEY_STEPS)
    return jnp.where(allowed, distance.astype(F32) * (slope * (-float(stride))), MASKED)


def rows_of(ref, starts, lanes):
    return jnp.concatenate([ref[pl.ds(aligned(s, SUB), SUB), lanes] for s in starts], axis=0)


def middle_starts(block, residue, chunks):
    tile = FAR_DILATION * SUB
    group = FAR_DILATION // MIDDLE_DILATION
    return [
        (block * chunks + s) * tile + (residue + MIDDLE_DILATION * b) * SUB
        for s in range(chunks)
        for b in range(group)
    ]


def far_starts(residue, chunks):
    return [g * FAR_DILATION * SUB + residue * SUB for g in range(chunks)]


def fold_in(refs, starts, lanes, new):
    size = SUB
    for n, start in enumerate(starts):
        where = (pl.ds(aligned(start, SUB), size), lanes)
        old = tuple(ref[where] for ref in refs)
        piece = tuple(item[n * size : (n + 1) * size] for item in new)
        for ref, value in zip(refs, merge(old, piece)):
            ref[where] = value


def pair_lanes(pair, offset=0):
    return slice(offset + pair * 128, offset + (pair + 1) * 128)


def bias_kernel(near, mid, far):
    heads = near.shape[0]
    y, _, tp = places()
    tile = FAR_DILATION * SUB
    chunks = mid.shape[1] // (tile // MIDDLE_DILATION)
    near_steps = near_distance(True, True)
    mid_steps = middle_distance(True, True, chunks)
    row = lax.broadcasted_iota(jnp.int32, far.shape[2:], 0)
    col = lax.broadcasted_iota(jnp.int32, far.shape[2:], 1)
    far_slope = lambda head, shape: jnp.exp2(
        jnp.full(shape, -ALIBI_EXP / HEADS, F32)
        * (tp * 2 * heads + (head // 2) * 4 + y * 2 + head % 2 + 1).astype(F32)
    ) * LOG2E
    for head in range(heads):
        slope = far_slope(head, (1, 1))
        near[head] = bias_of(near_steps, slope, 1)
        mid[head] = bias_of(mid_steps, slope, MIDDLE_DILATION)
        for back in range(3):
            far[back, head] = bias_of(row - col + back * far.shape[3], slope, FAR_DILATION)


def biases(block, heads):
    tile = FAR_DILATION * SUB
    size = block // MIDDLE_DILATION
    reach = 2 * block // FAR_DILATION
    return call(
        bias_kernel,
        [((heads, tile, 2 * tile), F32), ((heads, size, 2 * size), F32), ((3, heads, reach, reach), F32)],
        [],
        limit=8,
        flops=10**9,
        loose=0,
    )


def stacked(ref, pair, rows, columns, extra=None):
    both = jnp.concatenate([ref[2 * pair, rows, columns], ref[2 * pair + 1, rows, columns]], axis=0)
    return both if extra is None else both + extra


def closed_gate():
    _, z, _ = places()
    return jnp.where(z > 0, 0.0, MASKED).astype(F32)


def place_pair(target, mine, part):
    y, _, _ = places()
    block = mine.shape[0]
    target[pl.ds(aligned(y * block, block), block)] = mine[...]
    target[pl.ds(aligned((1 - y) * block, block), block)] = part[...]


KEYS, VALUES = slice(0, 128), slice(128, 256)


def block_kernel(near, mid, q, kv0, kv1, *rest):
    o_ref, m_ref, l_ref = rest[-3:]
    block = q.shape[0]
    tile = FAR_DILATION * SUB
    chunks = block // tile
    refs = (o_ref, m_ref, l_ref)
    step = 128
    size = mid.shape[1]
    for pair, kv in enumerate((kv0, kv1)):
        for index in range(chunks):
            first = max(index - 1, 0) * tile
            width = tile if index == 0 else 2 * tile
            columns = slice(2 * tile - width, 2 * tile)
            for inner in range(tile // step):
                start = index * tile + inner * step
                result = attend(
                    q[start : start + step, pair_lanes(pair)],
                    kv[first : first + width, KEYS],
                    kv[first : first + width, VALUES],
                    stacked(near, pair, slice(inner * step, (inner + 1) * step), columns),
                )
                for ref, value in zip(refs, result):
                    ref[start : start + step, pair_lanes(pair)] = value
        for residue in range(MIDDLE_DILATION):
            starts = middle_starts(0, residue, chunks)
            result = attend(
                rows_of(q, starts, pair_lanes(pair)),
                rows_of(kv, starts, KEYS),
                rows_of(kv, starts, VALUES),
                stacked(mid, pair, slice(0, size), slice(size, 2 * size)),
            )
            fold_in(refs, starts, pair_lanes(pair), result)


def block_attention(bias, q, kv0, kv1, after=()):
    return call(
        block_kernel,
        [(q.shape, F32)] * 3,
        [bias[0], bias[1], q, kv0, kv1, *after],
        limit=10,
        flops=4 * 10**9,
        loose=len(after),
    )


def windows(refs, q, kvs, near, mid, far, before, closed):
    block = q.shape[0] // 2
    tile = FAR_DILATION * SUB
    chunks = block // tile
    back = 1 if before else 0
    query_tile = 0 if before else chunks
    key_tile = (2 * chunks - 1 if before else chunks - 1) * tile
    step = 128
    size = mid.shape[1]
    for pair in range(len(kvs)):
        kv = kvs[pair]
        for residue in range(FAR_DILATION):
            starts = far_starts(residue, 2 * chunks)
            result = attend(
                rows_of(q, starts, pair_lanes(pair)),
                rows_of(kv, starts, KEYS),
                rows_of(kv, starts, VALUES),
                jnp.concatenate([far[back, 2 * pair], far[back, 2 * pair + 1]], axis=0) + closed,
            )
            fold_in(refs, starts, pair_lanes(pair), result)
        for inner in range(tile // step):
            start = query_tile * tile + inner * step
            result = attend(
                q[start : start + step, pair_lanes(pair)],
                kv[key_tile : key_tile + tile, KEYS],
                kv[key_tile : key_tile + tile, VALUES],
                stacked(near, pair, slice(inner * step, (inner + 1) * step), slice(0, tile), closed),
            )
            where = (slice(start, start + step), pair_lanes(pair))
            old = tuple(ref[where] for ref in refs)
            for ref, value in zip(refs, merge(old, result)):
                ref[where] = value
        for residue in range(MIDDLE_DILATION):
            starts = middle_starts(0 if before else 1, residue, chunks)
            key_starts = middle_starts(1 if before else 0, residue, chunks)
            result = attend(
                rows_of(q, starts, pair_lanes(pair)),
                rows_of(kv, key_starts, KEYS),
                rows_of(kv, key_starts, VALUES),
                stacked(mid, pair, slice(0, size), slice(0, size), closed),
            )
            fold_in(refs, starts, pair_lanes(pair), result)


def pair_kernel(near, mid, far, q_mine, q_part, *rest):
    kv_mine, kv_part, mine, part = rest[:2], rest[2:4], rest[4:7], rest[7:10]
    *refs, q_ref, kv = rest[-5:]
    place_pair(q_ref, q_mine, q_part)
    for n in range(2):
        place_pair(kv.at[n], kv_mine[n], kv_part[n])
    for ref, first, second in zip(refs, mine, part):
        place_pair(ref, first, second)
    windows(refs, q_ref, [kv.at[0], kv.at[1]], near, mid, far, False, 0.0)


def pair_attention(bias, q_mine, q_part, kv_mine, kv_part, mine, part, after=()):
    block, lanes = q_mine.shape
    return call(
        pair_kernel,
        [((2 * block, lanes), F32)] * 3 + [((2 * block, lanes), BF16)],
        [*bias, q_mine, q_part, *kv_mine, *kv_part, *mine, *part, *after],
        [pltpu.VMEM((2, 2 * block, 256), BF16)],
        limit=16,
        flops=4 * 10**9,
        loose=len(after),
    )


def before_kernel(near, mid, far, q, kv_a0, kv_b0, kv_a1, kv_b1, o_in, m_in, l_in, *rest):
    o_ref, m_ref, l_ref, past = rest[-4:]
    place_pair(past.at[0], kv_a0, kv_b0)
    place_pair(past.at[1], kv_a1, kv_b1)
    o_ref[...], m_ref[...], l_ref[...] = o_in[...], m_in[...], l_in[...]
    windows((o_ref, m_ref, l_ref), q, [past.at[0], past.at[1]], near, mid, far, True, closed_gate())


def before_attention(bias, q, past, state, after=()):
    return call(
        before_kernel,
        [(q.shape, F32)] * 3,
        [*bias, q, *past, *state, *after],
        [pltpu.VMEM((2, q.shape[0], 256), BF16)],
        limit=16,
        flops=4 * 10**9,
        loose=len(after),
    )


def part_row(shape, block):
    row = lax.broadcasted_iota(jnp.int32, shape, 0) - 8 * block
    lane = lax.broadcasted_iota(jnp.int32, shape, 1)
    return row, lane


def pack_sums(blocks):
    total = 0.0
    for n, sums in enumerate(blocks):
        row, lane = part_row((16, 128), n)
        for part in range(3):
            piece = sums.astype(BF16)
            sums = sums - piece.astype(F32)
            pick = (row // 2 == part) & (row >= 0) & (lane == (row % 2) * HEAD_DIM)
            total = total + lax.dot_general(
                jnp.where(pick, 1.0, 0.0).astype(BF16), piece, (((1,), (1,)), ((), ())), preferred_element_type=F32
            )
    return total.astype(BF16)


def unpack_sums(packed, block):
    row, lane = part_row((16, 128), block)
    pick = (row >= 0) & (row < 6) & (lane // HEAD_DIM == row % 2)
    return lax.dot_general(
        packed, jnp.where(pick, 1.0, 0.0).astype(BF16), (((0,), (0,)), ((), ())), preferred_element_type=F32
    )


def store_packed(ref, first, packed):
    for n in range(packed.shape[1] // 128):
        ref[first + 16 * n : first + 16 * (n + 1)] = packed[:, n * 128 : (n + 1) * 128]


def load_packed(ref, first, count):
    return jnp.concatenate([ref[first + 16 * n : first + 16 * (n + 1)] for n in range(count)], axis=1)


def remote_kernel(pair, far, q_a, q_b, kv_a, kv_b, *rest):
    out_ref, q, kv, sums = rest[-4:]
    block = q_a.shape[0]
    tile = FAR_DILATION * SUB
    chunks = block // tile
    place_pair(q, q_a.at[:, pair_lanes(pair)], q_b.at[:, pair_lanes(pair)])
    place_pair(kv, kv_a, kv_b)
    closed = closed_gate()
    bias = jnp.concatenate([far[2, 2 * pair], far[2, 2 * pair + 1]], axis=0) + closed
    for residue in range(FAR_DILATION):
        starts = far_starts(residue, 2 * chunks)
        o, m, l = attend(rows_of(q, starts, KEYS), rows_of(kv, starts, KEYS), rows_of(kv, starts, VALUES), bias)
        some = l > 0.0
        safe = jnp.where(some, l, 1.0)
        o = o / safe
        s = jnp.where(some, m + jnp.log2(safe), FLOOR)
        for n, start in enumerate(starts):
            where = pl.ds(start, SUB)
            out_ref[where] = o[n * SUB : (n + 1) * SUB].astype(BF16)
            sums[where] = s[n * SUB : (n + 1) * SUB]
    store_packed(out_ref, 2 * block, pack_sums([sums[:block], sums[block:]]))


def remote_attention(pair, far, q_a, q_b, kv_a, kv_b, after=()):
    block = q_a.shape[0]
    return call(
        functools.partial(remote_kernel, pair),
        [((2 * block + 16 * (block // 128), 128), BF16)],
        [far, q_a, q_b, kv_a, kv_b, *after],
        [pltpu.VMEM((2 * block, 128), BF16), pltpu.VMEM((2 * block, 256), BF16), pltpu.VMEM((2 * block, 128), F32)],
        limit=8,
        flops=10**9,
        loose=len(after),
    )[0]


def finish_kernel(pair, o_in, m_in, l_in, far_in, *rest):
    stay_ref, go_ref, same_ref, cross_ref, sums_ref, o_s, turned = rest[-7:]
    y, _, tp = places()
    rows = o_in.shape[0]
    block = rows // 2
    half = block // 2
    tile = FAR_DILATION * SUB
    lanes = pair_lanes(pair)
    closed = closed_gate()
    packed = load_packed(far_in, rows, block // 128)
    for b in range(2):
        far_sums = unpack_sums(packed, b) + closed
        select = slice(b * block, (b + 1) * block)
        o, m, l = merge(
            (o_in[select, lanes], m_in[select, lanes], l_in[select, lanes]),
            (far_in[select].astype(F32), far_sums, jnp.ones_like(far_sums)),
        )
        o_s[0, select] = o / l
        o_s[1, select] = (m + jnp.log2(l)) * LN2
    for item in range(2):
        for s in range(rows // tile):
            for residue in range(FAR_DILATION):
                turned[item, pl.ds(s * tile + residue, SUB, stride=FAR_DILATION), :] = o_s[
                    item, s * tile + residue * SUB : s * tile + (residue + 1) * SUB
                ]
    own, other = y * block, (1 - y) * block
    for ref, start in (
        (stay_ref, own + tp * half),
        (go_ref, own + (1 - tp) * half),
        (same_ref, other + tp * half),
        (cross_ref, other + (1 - tp) * half),
    ):
        ref[:half] = turned[0, pl.ds(aligned(start, half), half), :].astype(BF16)
    sums_ref[...] = pack_sums([turned[1, pl.ds(aligned(own, block), block), :]])
    store_packed(same_ref, half, pack_sums([turned[1, pl.ds(aligned(other, block), block), :]]))


def finish(pair, state, far, after=()):
    rows = state[0].shape[0]
    block, half = rows // 2, rows // 4
    piece = ((half, 128), BF16)
    return call(
        functools.partial(finish_kernel, pair),
        [piece, piece, ((half + 16 * (block // 128), 128), BF16), piece, ((16, block), BF16)],
        [*state, far, *after],
        [pltpu.VMEM((2, rows, 128), F32), pltpu.VMEM((2, rows, 128), F32)],
        limit=8,
        flops=10**9,
        loose=len(after),
    )


def output_kernel(*refs):
    pieces, (w_mine, w_other, out_ref, sums_ref) = (refs[:5], refs[5:10]), refs[10:]
    y, _, _ = places()
    half, width = out_ref.shape
    block = 2 * half
    low = y == 0
    order = lambda mine, part: (jnp.where(low, mine, part), jnp.where(low, part, mine))
    hidden = []
    for first, second in ((0, 1), (2, 3)):
        blocks = []
        for piece in pieces:
            blocks += order(piece[first][:half], piece[second][:half])
        hidden.append(jnp.concatenate(blocks, axis=1))
    step = 512
    for start in range(0, width, step):
        columns = slice(start, start + step)
        first = jnp.dot(hidden[0], w_mine[:, columns], preferred_element_type=F32)
        second = jnp.dot(hidden[1], w_other[:, columns], preferred_element_type=F32)
        out_ref[:, columns] = (first.astype(BF16).astype(F32) + second.astype(BF16).astype(F32)).astype(BF16)
    heads = []
    for piece in pieces:
        sums = []
        for packed in (piece[4][...], load_packed(piece[1], half, block // 128)):
            packed = packed.astype(F32)
            sums.append(packed[0:2] + packed[2:4] + packed[4:6])
        heads += order(*sums)
    sums_ref[...] = jnp.concatenate(heads, axis=0)


def output(pieces, w_mine, w_other):
    half = pieces[0][0].shape[0]
    width = w_mine.shape[1]
    return call(
        output_kernel,
        [((half, width), BF16), ((8, 2 * half), F32)],
        [*pieces[0], *pieces[1], w_mine, w_other],
        limit=12,
        flops=2 * half * width * 1024,
    )


def layer(tokens, w_query, w_key, w_value, w_out):
    half, _ = tokens.shape
    block = 2 * half
    width = w_query.shape[1]
    heads = width // 2 // HEAD_DIM
    count = lax.axis_size("sp")
    assert lax.axis_size("tp") == 2 and count % 2 == 0
    assert REACH == 4 * block and half == FAR_DILATION * SUB and width == 512
    ahead = [(n, (n + 2) % count) for n in range(count)]
    back = [(n + 2, n) for n in range(count - 2)]
    onward = [(n, n + 2) for n in range(count - 2)]
    beside = [(n, n ^ 1) for n in range(count)]
    swap = [(0, 1), (1, 0)]
    crossed = [(2 * n + c, 2 * (n ^ 1) + 1 - c) for n in range(count) for c in range(2)]

    x_other = lax.ppermute(tokens, "tp", swap)
    kv_t0, kv_m0 = project(tokens, x_other, [w_key, w_value], [0])
    kv_p0 = lax.ppermute(kv_t0, "sp", beside)
    kv_a0 = lax.ppermute(kv_m0, "sp", ahead)
    q_t, q_m = project(tokens, x_other, [w_query], [0, 256])
    q_p = lax.ppermute(q_t, "sp", beside)
    q_a = lax.ppermute(q_m, "sp", back)
    kv_t1, kv_m1 = project(tokens, x_other, [w_key, w_value], [256])
    kv_p1 = lax.ppermute(kv_t1, "sp", beside)
    kv_a1 = lax.ppermute(kv_m1, "sp", ahead)
    kv_b0 = lax.ppermute(kv_p0, "sp", onward)
    q_b = lax.ppermute(q_p, "sp", back)
    kv_b1 = lax.ppermute(kv_p1, "sp", onward)
    w_other = lax.ppermute(w_out, "tp", swap)
    bias = biases(block, heads)
    mine = block_attention(bias, q_m, kv_m0, kv_m1)
    part = block_attention(bias, q_p, kv_p0, kv_p1, mine[:1])
    far0 = remote_attention(0, bias[2], q_a, q_b, kv_a0, kv_b0)
    far_p = lax.ppermute(far0, "sp", ahead)
    *state, q = pair_attention(bias, q_m, q_p, (kv_m0, kv_m1), (kv_p0, kv_p1), mine, part)
    far1 = remote_attention(1, bias[2], q_a, q_b, kv_a1, kv_b1)
    far_m = lax.ppermute(far1, "sp", ahead)
    state = before_attention(bias, q, (kv_a0, kv_b0, kv_a1, kv_b1), state)
    pieces = []
    for pair, far in enumerate((far_p, far_m)):
        stay, go, same, cross, sums = finish(pair, state, far)
        same = lax.ppermute(same, "sp", beside)
        cross = lax.ppermute(cross, ("sp", "tp"), crossed)
        go = lax.ppermute(go, "tp", swap)
        pieces.append((stay, same, go, cross, sums))
    return output(pieces, w_out, w_other)


def solution(mesh):
    in_specs = (
        P(("grp", "sp", "tp"), None),
        P(None, "tp"),
        P(None, "tp"),
        P(None, "tp"),
        P("tp", None),
    )
    out_specs = (P(("grp", "sp", "tp"), None), P("tp", ("grp", "sp")))
    return jax.shard_map(layer, mesh=mesh, in_specs=in_specs, out_specs=out_specs, check_vma=False)
```

```python
import functools
import math

import jax
import jax.numpy as jnp
from jax import lax
from jax.experimental import pallas as pl
from jax.experimental.pallas import tpu as pltpu
from jax.sharding import PartitionSpec as P


HEADS = 16
HEAD_DIM = 64
WINDOW_KEY_STEPS = 128
MIDDLE_DILATION = 4
FAR_DILATION = 16
REACH = 2048
ALIBI_EXP = 16.0

LOG2E = math.log2(math.e)
LN2 = math.log(2.0)
MASKED = -1e30
FLOOR = -1e25
F32 = jnp.float32
BF16 = jnp.bfloat16
ANY = pl.BlockSpec(memory_space=pl.ANY)
VMEM = pl.BlockSpec(memory_space=pltpu.VMEM)

MIB = 1024 * 1024


def params(limit):
    return pltpu.CompilerParams(vmem_limit_bytes=limit * MIB)


SUB = 16


def aligned(value, multiple):
    return value if isinstance(value, int) else pl.multiple_of(value, multiple)


def places():
    place = lax.axis_index("sp")
    return place % 2, place // 2, lax.axis_index("tp")


def call(kernel, results, inputs, scratch=(), limit=12, flops=10**9, loose=0):
    return pl.pallas_call(
        kernel,
        out_shape=[jax.ShapeDtypeStruct(shape, kind) for shape, kind in results],
        in_specs=[VMEM] * (len(inputs) - loose) + [ANY] * loose,
        out_specs=[VMEM] * len(results),
        scratch_shapes=list(scratch),
        compiler_params=params(limit),
        cost_estimate=pl.CostEstimate(flops=flops, bytes_accessed=10**6, transcendentals=0),
    )(*inputs)


def project_kernel(first, weights, *refs):
    x_own, x_other = refs[:2]
    ws = refs[2 : 2 + weights]
    outs, acc = refs[2 + weights : -1], refs[-1]
    y, _, tp = places()
    rows = x_own.shape[0]
    slot = 0
    for w in ws:
        for start in first:
            for half, x in enumerate((x_own, x_other)):
                result = jnp.dot(x[...], w[:, start : start + 256], preferred_element_type=F32)
                acc[slot, 0], acc[slot, 1] = result[:, :128], result[:, 128:]
                place = (tp if half == 0 else 1 - tp) * rows
                index = slot // 2 if len(first) > 1 or weights > 1 else 0
                for side, out in enumerate(outs):
                    source = 1 - y if side == 0 else y
                    for residue in range(FAR_DILATION):
                        chunk = acc[slot, source, pl.ds(residue, SUB, stride=FAR_DILATION), :].astype(BF16)
                        where = pl.ds(aligned(place + residue * SUB, SUB), SUB)
                        out[where, index * 128 : (index + 1) * 128] = chunk
                slot += 1


def project(x_own, x_other, weights, first):
    rows, width = x_own.shape
    shape = ((2 * rows, 256), BF16)
    slots = 2 * len(first) * len(weights)
    return call(
        functools.partial(project_kernel, first, len(weights)),
        [shape, shape],
        [x_own, x_other, *weights],
        [pltpu.VMEM((slots, 2, rows, 128), F32)],
        limit=10,
        flops=2 * slots * rows * width * 256,
    )


def attend(queries, keys, values, bias):
    rows = queries.shape[0]
    low = lax.broadcasted_iota(jnp.int32, (rows, 128), 1) < HEAD_DIM
    zero = jnp.zeros_like(queries)
    stacked = jnp.concatenate([jnp.where(low, queries, zero), jnp.where(low, zero, queries)], axis=0)
    scores = lax.dot_general(
        stacked, keys, (((1,), (1,)), ((), ())), preferred_element_type=F32
    )
    scores = scores * (HEAD_DIM**-0.5 * LOG2E) + bias
    maxima = jnp.maximum(jnp.max(scores, axis=1, keepdims=True), FLOOR)
    weights = jnp.exp2(scores - maxima)
    totals = jnp.sum(weights, axis=1, keepdims=True)
    summed = jnp.dot(weights.astype(BF16), values, preferred_element_type=F32)
    pick = lambda item: jnp.where(low, item[:rows], item[rows:])
    return pick(summed), pick(maxima), pick(totals)


def merge(first, second):
    o1, m1, l1 = first
    o2, m2, l2 = second
    top = jnp.maximum(m1, m2)
    a, b = jnp.exp2(m1 - top), jnp.exp2(m2 - top)
    return o1 * a + o2 * b, top, l1 * a + l2 * b


def near_distance(keys_before, keys_own):
    tile = FAR_DILATION * SUB
    token = lambda n: FAR_DILATION * (n % SUB) + n // SUB
    shape = (tile, (tile if keys_before else 0) + (tile if keys_own else 0))
    row = token(lax.broadcasted_iota(jnp.int32, shape, 0))
    col = lax.broadcasted_iota(jnp.int32, shape, 1)
    if keys_before:
        key = jnp.where(col < tile, token(col) - tile, token(col - tile))
    else:
        key = token(col)
    return row - key


def middle_distance(keys_before, keys_own, chunks):
    group = FAR_DILATION // MIDDLE_DILATION
    size = chunks * group * SUB
    step = lambda n: (n // (group * SUB)) * (group * SUB) + group * (n % SUB) + (n // SUB) % group
    shape = (size, (size if keys_before else 0) + (size if keys_own else 0))
    row = step(lax.broadcasted_iota(jnp.int32, shape, 0))
    col = lax.broadcasted_iota(jnp.int32, shape, 1)
    if keys_before:
        key = jnp.where(col < size, step(col) - size, step(col - size))
    else:
        key = step(col)
    return row - key


def bias_of(distance, slope, stride):
    allowed = (distance >= 0) & (distance <= WINDOW_KEY_STEPS)
    return jnp.where(allowed, distance.astype(F32) * (slope * (-float(stride))), MASKED)


def rows_of(ref, starts, lanes):
    return jnp.concatenate([ref[pl.ds(aligned(s, SUB), SUB), lanes] for s in starts], axis=0)


def middle_starts(block, residue, chunks):
    tile = FAR_DILATION * SUB
    group = FAR_DILATION // MIDDLE_DILATION
    return [
        (block * chunks + s) * tile + (residue + MIDDLE_DILATION * b) * SUB
        for s in range(chunks)
        for b in range(group)
    ]


def far_starts(residue, chunks):
    return [g * FAR_DILATION * SUB + residue * SUB for g in range(chunks)]


def fold_in(refs, starts, lanes, new):
    size = SUB
    for n, start in enumerate(starts):
        where = (pl.ds(aligned(start, SUB), size), lanes)
        old = tuple(ref[where] for ref in refs)
        piece = tuple(item[n * size : (n + 1) * size] for item in new)
        for ref, value in zip(refs, merge(old, piece)):
            ref[where] = value


def pair_lanes(pair, offset=0):
    return slice(offset + pair * 128, offset + (pair + 1) * 128)


def bias_kernel(near, mid, far):
    heads = near.shape[0]
    y, _, tp = places()
    tile = FAR_DILATION * SUB
    chunks = mid.shape[1] // (tile // MIDDLE_DILATION)
    near_steps = near_distance(True, True)
    mid_steps = middle_distance(True, True, chunks)
    row = lax.broadcasted_iota(jnp.int32, far.shape[2:], 0)
    col = lax.broadcasted_iota(jnp.int32, far.shape[2:], 1)
    far_slope = lambda head, shape: jnp.exp2(
        jnp.full(shape, -ALIBI_EXP / HEADS, F32)
        * (tp * 2 * heads + (head // 2) * 4 + y * 2 + head % 2 + 1).astype(F32)
    ) * LOG2E
    for head in range(heads):
        slope = far_slope(head, (1, 1))
        near[head] = bias_of(near_steps, slope, 1)
        mid[head] = bias_of(mid_steps, slope, MIDDLE_DILATION)
        for back in range(3):
            far[back, head] = bias_of(row - col + back * far.shape[3], slope, FAR_DILATION)


def biases(block, heads):
    tile = FAR_DILATION * SUB
    size = block // MIDDLE_DILATION
    reach = 2 * block // FAR_DILATION
    return call(
        bias_kernel,
        [((heads, tile, 2 * tile), F32), ((heads, size, 2 * size), F32), ((3, heads, reach, reach), F32)],
        [],
        limit=8,
        flops=10**9,
        loose=0,
    )


def stacked(ref, pair, rows, columns):
    return jnp.concatenate([ref[2 * pair, rows, columns], ref[2 * pair + 1, rows, columns]], axis=0)


def closed_gate():
    _, z, _ = places()
    return jnp.where(z > 0, 0.0, MASKED).astype(F32)


def place_pair(target, mine, part):
    y, _, _ = places()
    block = mine.shape[0]
    target[pl.ds(aligned(y * block, block), block)] = mine[...]
    target[pl.ds(aligned((1 - y) * block, block), block)] = part[...]


KEYS, VALUES = slice(0, 128), slice(128, 256)


def block_kernel(near, mid, q, kv0, kv1, *rest):
    o_ref, m_ref, l_ref = rest[-3:]
    block = q.shape[0]
    tile = FAR_DILATION * SUB
    chunks = block // tile
    refs = (o_ref, m_ref, l_ref)
    step = 128
    size = mid.shape[1]
    for pair, kv in enumerate((kv0, kv1)):
        for index in range(chunks):
            first = max(index - 1, 0) * tile
            width = tile if index == 0 else 2 * tile
            columns = slice(2 * tile - width, 2 * tile)
            for inner in range(tile // step):
                start = index * tile + inner * step
                result = attend(
                    q[start : start + step, pair_lanes(pair)],
                    kv[first : first + width, KEYS],
                    kv[first : first + width, VALUES],
                    stacked(near, pair, slice(inner * step, (inner + 1) * step), columns),
                )
                for ref, value in zip(refs, result):
                    ref[start : start + step, pair_lanes(pair)] = value
        for residue in range(MIDDLE_DILATION):
            starts = middle_starts(0, residue, chunks)
            result = attend(
                rows_of(q, starts, pair_lanes(pair)),
                rows_of(kv, starts, KEYS),
                rows_of(kv, starts, VALUES),
                stacked(mid, pair, slice(0, size), slice(size, 2 * size)),
            )
            fold_in(refs, starts, pair_lanes(pair), result)


def block_attention(bias, q, kv0, kv1, after=()):
    return call(
        block_kernel,
        [(q.shape, F32)] * 3,
        [bias[0], bias[1], q, kv0, kv1, *after],
        limit=10,
        flops=4 * 10**9,
        loose=len(after),
    )


def windows(refs, q, kvs, near, mid, far, before):
    block = q.shape[0] // 2
    tile = FAR_DILATION * SUB
    chunks = block // tile
    back = 1 if before else 0
    query_tile = 0 if before else chunks
    key_tile = (2 * chunks - 1 if before else chunks - 1) * tile
    step = 128
    size = mid.shape[1]
    for pair in range(len(kvs)):
        kv = kvs[pair]
        for residue in range(FAR_DILATION):
            starts = far_starts(residue, 2 * chunks)
            result = attend(
                rows_of(q, starts, pair_lanes(pair)),
                rows_of(kv, starts, KEYS),
                rows_of(kv, starts, VALUES),
                jnp.concatenate([far[back, 2 * pair], far[back, 2 * pair + 1]], axis=0),
            )
            fold_in(refs, starts, pair_lanes(pair), result)
        for inner in range(tile // step):
            start = query_tile * tile + inner * step
            result = attend(
                q[start : start + step, pair_lanes(pair)],
                kv[key_tile : key_tile + tile, KEYS],
                kv[key_tile : key_tile + tile, VALUES],
                stacked(near, pair, slice(inner * step, (inner + 1) * step), slice(0, tile)),
            )
            where = (slice(start, start + step), pair_lanes(pair))
            old = tuple(ref[where] for ref in refs)
            for ref, value in zip(refs, merge(old, result)):
                ref[where] = value
        for residue in range(MIDDLE_DILATION):
            starts = middle_starts(0 if before else 1, residue, chunks)
            key_starts = middle_starts(1 if before else 0, residue, chunks)
            result = attend(
                rows_of(q, starts, pair_lanes(pair)),
                rows_of(kv, key_starts, KEYS),
                rows_of(kv, key_starts, VALUES),
                stacked(mid, pair, slice(0, size), slice(0, size)),
            )
            fold_in(refs, starts, pair_lanes(pair), result)


def pair_kernel(near, mid, far, q_mine, q_part, *rest):
    kv_mine, kv_part, mine, part = rest[:2], rest[2:4], rest[4:7], rest[7:10]
    *refs, q_ref, kv = rest[-5:]
    place_pair(q_ref, q_mine, q_part)
    for n in range(2):
        place_pair(kv.at[n], kv_mine[n], kv_part[n])
    for ref, first, second in zip(refs, mine, part):
        place_pair(ref, first, second)
    windows(refs, q_ref, [kv.at[0], kv.at[1]], near, mid, far, False)


def pair_attention(bias, q_mine, q_part, kv_mine, kv_part, mine, part, after=()):
    block, lanes = q_mine.shape
    return call(
        pair_kernel,
        [((2 * block, lanes), F32)] * 3 + [((2 * block, lanes), BF16)],
        [*bias, q_mine, q_part, *kv_mine, *kv_part, *mine, *part, *after],
        [pltpu.VMEM((2, 2 * block, 256), BF16)],
        limit=16,
        flops=4 * 10**9,
        loose=len(after),
    )


def before_kernel(near, mid, far, q, kv_a0, kv_b0, kv_a1, kv_b1, o_in, m_in, l_in, *rest):
    o_ref, m_ref, l_ref, past = rest[-4:]
    o_ref[...], m_ref[...], l_ref[...] = o_in[...], m_in[...], l_in[...]

    @pl.when(places()[1] > 0)
    def _():
        place_pair(past.at[0], kv_a0, kv_b0)
        place_pair(past.at[1], kv_a1, kv_b1)
        windows((o_ref, m_ref, l_ref), q, [past.at[0], past.at[1]], near, mid, far, True)


def before_attention(bias, q, past, state, after=()):
    return call(
        before_kernel,
        [(q.shape, F32)] * 3,
        [*bias, q, *past, *state, *after],
        [pltpu.VMEM((2, q.shape[0], 256), BF16)],
        limit=16,
        flops=4 * 10**9,
        loose=len(after),
    )


def part_row(shape, block):
    row = lax.broadcasted_iota(jnp.int32, shape, 0) - 8 * block
    lane = lax.broadcasted_iota(jnp.int32, shape, 1)
    return row, lane


def pack_sums(blocks):
    total = 0.0
    for n, sums in enumerate(blocks):
        row, lane = part_row((16, 128), n)
        for part in range(3):
            piece = sums.astype(BF16)
            sums = sums - piece.astype(F32)
            pick = (row // 2 == part) & (row >= 0) & (lane == (row % 2) * HEAD_DIM)
            total = total + lax.dot_general(
                jnp.where(pick, 1.0, 0.0).astype(BF16), piece, (((1,), (1,)), ((), ())), preferred_element_type=F32
            )
    return total.astype(BF16)


def unpack_sums(packed, block):
    row, lane = part_row((16, 128), block)
    pick = (row >= 0) & (row < 6) & (lane // HEAD_DIM == row % 2)
    return lax.dot_general(
        packed, jnp.where(pick, 1.0, 0.0).astype(BF16), (((0,), (0,)), ((), ())), preferred_element_type=F32
    )


def store_packed(ref, first, packed):
    for n in range(packed.shape[1] // 128):
        ref[first + 16 * n : first + 16 * (n + 1)] = packed[:, n * 128 : (n + 1) * 128]


def load_packed(ref, first, count):
    return jnp.concatenate([ref[first + 16 * n : first + 16 * (n + 1)] for n in range(count)], axis=1)


def remote_kernel(pair, far, q_a, q_b, kv_a, kv_b, *rest):
    out_ref, q, kv, sums = rest[-4:]
    block = q_a.shape[0]
    tile = FAR_DILATION * SUB
    chunks = block // tile
    _, z, _ = places()
    useful = (z > 0) & (z + 1 < lax.axis_size("sp") // 2)

    @pl.when(useful)
    def _():
        place_pair(q, q_a.at[:, pair_lanes(pair)], q_b.at[:, pair_lanes(pair)])
        place_pair(kv, kv_a, kv_b)
        bias = jnp.concatenate([far[2, 2 * pair], far[2, 2 * pair + 1]], axis=0)
        for residue in range(FAR_DILATION):
            starts = far_starts(residue, 2 * chunks)
            o, m, l = attend(rows_of(q, starts, KEYS), rows_of(kv, starts, KEYS), rows_of(kv, starts, VALUES), bias)
            some = l > 0.0
            safe = jnp.where(some, l, 1.0)
            o = o / safe
            s = jnp.where(some, m + jnp.log2(safe), FLOOR)
            for n, start in enumerate(starts):
                where = pl.ds(start, SUB)
                out_ref[where] = o[n * SUB : (n + 1) * SUB].astype(BF16)
                sums[where] = s[n * SUB : (n + 1) * SUB]
        store_packed(out_ref, 2 * block, pack_sums([sums[:block], sums[block:]]))

    @pl.when(jnp.logical_not(useful))
    def _():
        out_ref[: 2 * block] = jnp.zeros((2 * block, 128), BF16)
        store_packed(out_ref, 2 * block, pack_sums([jnp.full((block, 128), FLOOR, F32)] * 2))


def remote_attention(pair, far, q_a, q_b, kv_a, kv_b, after=()):
    block = q_a.shape[0]
    return call(
        functools.partial(remote_kernel, pair),
        [((2 * block + 16 * (block // 128), 128), BF16)],
        [far, q_a, q_b, kv_a, kv_b, *after],
        [pltpu.VMEM((2 * block, 128), BF16), pltpu.VMEM((2 * block, 256), BF16), pltpu.VMEM((2 * block, 128), F32)],
        limit=8,
        flops=10**9,
        loose=len(after),
    )[0]


def finish_kernel(pair, o_in, m_in, l_in, far_in, *rest):
    stay_ref, go_ref, same_ref, cross_ref, sums_ref, o_s, turned = rest[-7:]
    y, _, tp = places()
    rows = o_in.shape[0]
    block = rows // 2
    half = block // 2
    tile = FAR_DILATION * SUB
    lanes = pair_lanes(pair)
    closed = closed_gate()
    packed = load_packed(far_in, rows, block // 128)
    for b in range(2):
        far_sums = unpack_sums(packed, b) + closed
        select = slice(b * block, (b + 1) * block)
        o, m, l = merge(
            (o_in[select, lanes], m_in[select, lanes], l_in[select, lanes]),
            (far_in[select].astype(F32), far_sums, jnp.ones_like(far_sums)),
        )
        o_s[0, select] = o / l
        o_s[1, select] = (m + jnp.log2(l)) * LN2
    for item in range(2):
        for s in range(rows // tile):
            for residue in range(FAR_DILATION):
                turned[item, pl.ds(s * tile + residue, SUB, stride=FAR_DILATION), :] = o_s[
                    item, s * tile + residue * SUB : s * tile + (residue + 1) * SUB
                ]
    own, other = y * block, (1 - y) * block
    for ref, start in (
        (stay_ref, own + tp * half),
        (go_ref, own + (1 - tp) * half),
        (same_ref, other + tp * half),
        (cross_ref, other + (1 - tp) * half),
    ):
        ref[:half] = turned[0, pl.ds(aligned(start, half), half), :].astype(BF16)
    sums_ref[...] = pack_sums([turned[1, pl.ds(aligned(own, block), block), :]])
    store_packed(same_ref, half, pack_sums([turned[1, pl.ds(aligned(other, block), block), :]]))


def finish(pair, state, far, after=()):
    rows = state[0].shape[0]
    block, half = rows // 2, rows // 4
    piece = ((half, 128), BF16)
    return call(
        functools.partial(finish_kernel, pair),
        [piece, piece, ((half + 16 * (block // 128), 128), BF16), piece, ((16, block), BF16)],
        [*state, far, *after],
        [pltpu.VMEM((2, rows, 128), F32), pltpu.VMEM((2, rows, 128), F32)],
        limit=8,
        flops=10**9,
        loose=len(after),
    )


def output_kernel(*refs):
    pieces, (w_mine, w_other, out_ref, sums_ref) = (refs[:5], refs[5:10]), refs[10:]
    y, _, _ = places()
    half, width = out_ref.shape
    block = 2 * half
    low = y == 0
    order = lambda mine, part: (jnp.where(low, mine, part), jnp.where(low, part, mine))
    hidden = []
    for first, second in ((0, 1), (2, 3)):
        blocks = []
        for piece in pieces:
            blocks += order(piece[first][:half], piece[second][:half])
        hidden.append(jnp.concatenate(blocks, axis=1))
    step = 512
    for start in range(0, width, step):
        columns = slice(start, start + step)
        first = jnp.dot(hidden[0], w_mine[:, columns], preferred_element_type=F32)
        second = jnp.dot(hidden[1], w_other[:, columns], preferred_element_type=F32)
        out_ref[:, columns] = (first.astype(BF16).astype(F32) + second.astype(BF16).astype(F32)).astype(BF16)
    heads = []
    for piece in pieces:
        sums = []
        for packed in (piece[4][...], load_packed(piece[1], half, block // 128)):
            packed = packed.astype(F32)
            sums.append(packed[0:2] + packed[2:4] + packed[4:6])
        heads += order(*sums)
    sums_ref[...] = jnp.concatenate(heads, axis=0)


def output(pieces, w_mine, w_other):
    half = pieces[0][0].shape[0]
    width = w_mine.shape[1]
    return call(
        output_kernel,
        [((half, width), BF16), ((8, 2 * half), F32)],
        [*pieces[0], *pieces[1], w_mine, w_other],
        limit=12,
        flops=2 * half * width * 1024,
    )


def layer(tokens, w_query, w_key, w_value, w_out):
    half, _ = tokens.shape
    block = 2 * half
    width = w_query.shape[1]
    heads = width // 2 // HEAD_DIM
    count = lax.axis_size("sp")
    assert lax.axis_size("tp") == 2 and count % 2 == 0
    assert REACH == 4 * block and half == FAR_DILATION * SUB and width == 512
    ahead = [(n, (n + 2) % count) for n in range(count)]
    back = [(n + 2, n) for n in range(count - 2)]
    onward = [(n, n + 2) for n in range(count - 2)]
    beside = [(n, n ^ 1) for n in range(count)]
    swap = [(0, 1), (1, 0)]
    crossed = [(2 * n + c, 2 * (n ^ 1) + 1 - c) for n in range(count) for c in range(2)]

    x_other = lax.ppermute(tokens, "tp", swap)
    kv_t0, kv_m0 = project(tokens, x_other, [w_key[:, :256], w_value[:, :256]], [0])
    kv_p0 = lax.ppermute(kv_t0, "sp", beside)
    kv_a0 = lax.ppermute(kv_m0, "sp", ahead)
    q_t, q_m = project(tokens, x_other, [w_query], [0, 256])
    q_p = lax.ppermute(q_t, "sp", beside)
    q_a = lax.ppermute(q_m, "sp", back)
    kv_t1, kv_m1 = project(tokens, x_other, [w_key, w_value], [256])
    kv_p1 = lax.ppermute(kv_t1, "sp", beside)
    kv_a1 = lax.ppermute(kv_m1, "sp", ahead)
    kv_b0 = lax.ppermute(kv_p0, "sp", onward)
    q_b = lax.ppermute(q_p, "sp", back)
    kv_b1 = lax.ppermute(kv_p1, "sp", onward)
    w_other = lax.ppermute(w_out, "tp", swap)
    bias = biases(block, heads)
    mine = block_attention(bias, q_m, kv_m0, kv_m1)
    part = block_attention(bias, q_p, kv_p0, kv_p1, mine[:1])
    far0 = remote_attention(0, bias[2], q_a, q_b, kv_a0, kv_b0)
    far_p = lax.ppermute(far0, "sp", ahead)
    *state, q = pair_attention(bias, q_m, q_p, (kv_m0, kv_m1), (kv_p0, kv_p1), mine, part)
    far1 = remote_attention(1, bias[2], q_a, q_b, kv_a1, kv_b1)
    far_m = lax.ppermute(far1, "sp", onward)
    state = before_attention(bias, q, (kv_a0, kv_b0, kv_a1, kv_b1), state)
    pieces = []
    for pair, far in enumerate((far_p, far_m)):
        stay, go, same, cross, sums = finish(pair, state, far)
        same = lax.ppermute(same, "sp", beside)
        cross = lax.ppermute(cross, ("sp", "tp"), crossed)
        go = lax.ppermute(go, "tp", swap)
        pieces.append((stay, same, go, cross, sums))
    return output(pieces, w_out, w_other)


def solution(mesh):
    in_specs = (
        P(("grp", "sp", "tp"), None),
        P(None, "tp"),
        P(None, "tp"),
        P(None, "tp"),
        P("tp", None),
    )
    out_specs = (P(("grp", "sp", "tp"), None), P("tp", ("grp", "sp")))
    return jax.shard_map(layer, mesh=mesh, in_specs=in_specs, out_specs=out_specs, check_vma=False)
```

```python
import functools
import math

import jax
import jax.numpy as jnp
from jax import lax
from jax.experimental import pallas as pl
from jax.experimental.pallas import tpu as pltpu
from jax.sharding import PartitionSpec as P


HEADS = 16
HEAD_DIM = 64
WINDOW_KEY_STEPS = 128
MIDDLE_DILATION = 4
FAR_DILATION = 16
REACH = 2048
ALIBI_EXP = 16.0

LOG2E = math.log2(math.e)
LN2 = math.log(2.0)
MASKED = -1e30
FLOOR = -1e25
F32 = jnp.float32
BF16 = jnp.bfloat16
ANY = pl.BlockSpec(memory_space=pl.ANY)
VMEM = pl.BlockSpec(memory_space=pltpu.VMEM)

MIB = 1024 * 1024


def params(limit):
    return pltpu.CompilerParams(vmem_limit_bytes=limit * MIB)


SUB = 16


def aligned(value, multiple):
    return value if isinstance(value, int) else pl.multiple_of(value, multiple)


def places():
    place = lax.axis_index("sp")
    return place % 2, place // 2, lax.axis_index("tp")


def call(kernel, results, inputs, scratch=(), limit=12, flops=10**9, loose=0):
    return pl.pallas_call(
        kernel,
        out_shape=[jax.ShapeDtypeStruct(shape, kind) for shape, kind in results],
        in_specs=[VMEM] * (len(inputs) - loose) + [ANY] * loose,
        out_specs=[VMEM] * len(results),
        scratch_shapes=list(scratch),
        compiler_params=params(limit),
        cost_estimate=pl.CostEstimate(flops=flops, bytes_accessed=10**6, transcendentals=0),
    )(*inputs)


def project_kernel(first, weights, *refs):
    x_own, x_other = refs[:2]
    ws = refs[2 : 2 + weights]
    outs, acc = refs[2 + weights : -1], refs[-1]
    y, _, tp = places()
    rows = x_own.shape[0]
    slot = 0
    for w in ws:
        for start in first:
            for half, x in enumerate((x_own, x_other)):
                result = jnp.dot(x[...], w[:, start : start + 256], preferred_element_type=F32)
                acc[slot, 0], acc[slot, 1] = result[:, :128], result[:, 128:]
                place = (tp if half == 0 else 1 - tp) * rows
                index = slot // 2 if len(first) > 1 or weights > 1 else 0
                for side, out in enumerate(outs):
                    source = 1 - y if side == 0 else y
                    for residue in range(FAR_DILATION):
                        chunk = acc[slot, source, pl.ds(residue, SUB, stride=FAR_DILATION), :].astype(BF16)
                        where = pl.ds(aligned(place + residue * SUB, SUB), SUB)
                        out[where, index * 128 : (index + 1) * 128] = chunk
                slot += 1


def project(x_own, x_other, weights, first):
    rows, width = x_own.shape
    shape = ((2 * rows, 256), BF16)
    slots = 2 * len(first) * len(weights)
    return call(
        functools.partial(project_kernel, first, len(weights)),
        [shape, shape],
        [x_own, x_other, *weights],
        [pltpu.VMEM((slots, 2, rows, 128), F32)],
        limit=10,
        flops=2 * slots * rows * width * 256,
    )


def attend(queries, keys, values, bias):
    rows = queries.shape[0]
    low = lax.broadcasted_iota(jnp.int32, (rows, 128), 1) < HEAD_DIM
    zero = jnp.zeros_like(queries)
    stacked = jnp.concatenate([jnp.where(low, queries, zero), jnp.where(low, zero, queries)], axis=0)
    scores = lax.dot_general(
        stacked, keys, (((1,), (1,)), ((), ())), preferred_element_type=F32
    )
    scores = scores * (HEAD_DIM**-0.5 * LOG2E) + bias
    maxima = jnp.maximum(jnp.max(scores, axis=1, keepdims=True), FLOOR)
    weights = jnp.exp2(scores - maxima)
    totals = jnp.sum(weights, axis=1, keepdims=True)
    summed = jnp.dot(weights.astype(BF16), values, preferred_element_type=F32)
    pick = lambda item: jnp.where(low, item[:rows], item[rows:])
    return pick(summed), pick(maxima), pick(totals)


def merge(first, second):
    o1, m1, l1 = first
    o2, m2, l2 = second
    top = jnp.maximum(m1, m2)
    a, b = jnp.exp2(m1 - top), jnp.exp2(m2 - top)
    return o1 * a + o2 * b, top, l1 * a + l2 * b


HALF = FAR_DILATION * SUB // 2


def half_token(row, half):
    size = SUB // 2
    return FAR_DILATION * (size * half + row % size) + row // size


def near_distance(half):
    shape = (HALF, 2 * HALF)
    row = half_token(lax.broadcasted_iota(jnp.int32, shape, 0), half)
    col = lax.broadcasted_iota(jnp.int32, shape, 1)
    if half == 0:
        key = jnp.where(col < HALF, half_token(col, 1) - 2 * HALF, half_token(col - HALF, 0))
    else:
        key = jnp.where(col < HALF, half_token(col, 0), half_token(col - HALF, 1))
    return row - key


def halves(ref, start, lanes):
    rows = ref[pl.ds(start, 2 * HALF), lanes].astype(F32)
    size = SUB // 2
    return [
        jnp.concatenate([rows[n * SUB + h * size : n * SUB + (h + 1) * size] for n in range(FAR_DILATION)], axis=0).astype(BF16)
        for h in range(2)
    ]


def half_rows(start, half):
    size = SUB // 2
    return [slice(start + n * SUB + half * size, start + n * SUB + (half + 1) * size) for n in range(FAR_DILATION)]


def near_bias(near, pair, half, columns):
    return jnp.concatenate([near[2 * pair, half, :, columns], near[2 * pair + 1, half, :, columns]], axis=0)


def middle_distance(keys_before, keys_own, chunks):
    group = FAR_DILATION // MIDDLE_DILATION
    size = chunks * group * SUB
    step = lambda n: (n // (group * SUB)) * (group * SUB) + group * (n % SUB) + (n // SUB) % group
    shape = (size, (size if keys_before else 0) + (size if keys_own else 0))
    row = step(lax.broadcasted_iota(jnp.int32, shape, 0))
    col = lax.broadcasted_iota(jnp.int32, shape, 1)
    if keys_before:
        key = jnp.where(col < size, step(col) - size, step(col - size))
    else:
        key = step(col)
    return row - key


def bias_of(distance, slope, stride):
    allowed = (distance >= 0) & (distance <= WINDOW_KEY_STEPS)
    return jnp.where(allowed, distance.astype(F32) * (slope * (-float(stride))), MASKED)


def rows_of(ref, starts, lanes):
    return jnp.concatenate([ref[pl.ds(aligned(s, SUB), SUB), lanes] for s in starts], axis=0)


def middle_starts(block, residue, chunks):
    tile = FAR_DILATION * SUB
    group = FAR_DILATION // MIDDLE_DILATION
    return [
        (block * chunks + s) * tile + (residue + MIDDLE_DILATION * b) * SUB
        for s in range(chunks)
        for b in range(group)
    ]


def far_starts(residue, chunks):
    return [g * FAR_DILATION * SUB + residue * SUB for g in range(chunks)]


def fold_in(refs, starts, lanes, new):
    size = SUB
    for n, start in enumerate(starts):
        where = (pl.ds(aligned(start, SUB), size), lanes)
        old = tuple(ref[where] for ref in refs)
        piece = tuple(item[n * size : (n + 1) * size] for item in new)
        for ref, value in zip(refs, merge(old, piece)):
            ref[where] = value


def pair_lanes(pair, offset=0):
    return slice(offset + pair * 128, offset + (pair + 1) * 128)


def bias_kernel(near, mid, far):
    heads = near.shape[0]
    y, _, tp = places()
    tile = FAR_DILATION * SUB
    chunks = mid.shape[1] // (tile // MIDDLE_DILATION)
    near_steps = [near_distance(half) for half in range(2)]
    mid_steps = middle_distance(True, True, chunks)
    row = lax.broadcasted_iota(jnp.int32, far.shape[2:], 0)
    col = lax.broadcasted_iota(jnp.int32, far.shape[2:], 1)
    far_slope = lambda head, shape: jnp.exp2(
        jnp.full(shape, -ALIBI_EXP / HEADS, F32)
        * (tp * 2 * heads + (head // 2) * 4 + y * 2 + head % 2 + 1).astype(F32)
    ) * LOG2E
    for head in range(heads):
        slope = far_slope(head, (1, 1))
        for half in range(2):
            near[head, half] = bias_of(near_steps[half], slope, 1)
        mid[head] = bias_of(mid_steps, slope, MIDDLE_DILATION)
        for back in range(3):
            far[back, head] = bias_of(row - col + back * far.shape[3], slope, FAR_DILATION)


def biases(block, heads):
    size = block // MIDDLE_DILATION
    reach = 2 * block // FAR_DILATION
    return call(
        bias_kernel,
        [((heads, 2, HALF, 2 * HALF), F32), ((heads, size, 2 * size), F32), ((3, heads, reach, reach), F32)],
        [],
        limit=8,
        flops=10**9,
        loose=0,
    )


def stacked(ref, pair, rows, columns):
    return jnp.concatenate([ref[2 * pair, rows, columns], ref[2 * pair + 1, rows, columns]], axis=0)


def closed_gate():
    _, z, _ = places()
    return jnp.where(z > 0, 0.0, MASKED).astype(F32)


def place_pair(target, mine, part):
    y, _, _ = places()
    block = mine.shape[0]
    target[pl.ds(aligned(y * block, block), block)] = mine[...]
    target[pl.ds(aligned((1 - y) * block, block), block)] = part[...]


KEYS, VALUES = slice(0, 128), slice(128, 256)


def block_kernel(near, mid, q, kv0, kv1, *rest):
    o_ref, m_ref, l_ref = rest[-3:]
    block = q.shape[0]
    tile = FAR_DILATION * SUB
    chunks = block // tile
    refs = (o_ref, m_ref, l_ref)
    size = mid.shape[1]
    for pair, kv in enumerate((kv0, kv1)):
        earlier = None
        for index in range(chunks):
            start = index * tile
            queries = halves(q, start, pair_lanes(pair))
            keys, values = halves(kv, start, KEYS), halves(kv, start, VALUES)
            for half in range(2):
                if half == 1:
                    seen_keys, seen_values, columns = keys, values, slice(0, tile)
                elif earlier is None:
                    seen_keys, seen_values, columns = keys[:1], values[:1], slice(HALF, tile)
                else:
                    seen_keys, seen_values = [earlier[0], keys[0]], [earlier[1], values[0]]
                    columns = slice(0, tile)
                result = attend(
                    queries[half],
                    jnp.concatenate(seen_keys, axis=0),
                    jnp.concatenate(seen_values, axis=0),
                    near_bias(near, pair, half, columns),
                )
                for n, rows in enumerate(half_rows(start, half)):
                    for ref, value in zip(refs, result):
                        ref[rows, pair_lanes(pair)] = value[n * SUB // 2 : (n + 1) * SUB // 2]
            earlier = (keys[1], values[1])
        for residue in range(MIDDLE_DILATION):
            starts = middle_starts(0, residue, chunks)
            result = attend(
                rows_of(q, starts, pair_lanes(pair)),
                rows_of(kv, starts, KEYS),
                rows_of(kv, starts, VALUES),
                stacked(mid, pair, slice(0, size), slice(size, 2 * size)),
            )
            fold_in(refs, starts, pair_lanes(pair), result)


def block_attention(bias, q, kv0, kv1, after=()):
    return call(
        block_kernel,
        [(q.shape, F32)] * 3,
        [bias[0], bias[1], q, kv0, kv1, *after],
        limit=10,
        flops=4 * 10**9,
        loose=len(after),
    )


def windows(refs, q, kvs, near, mid, far, before):
    block = q.shape[0] // 2
    tile = FAR_DILATION * SUB
    chunks = block // tile
    back = 1 if before else 0
    query_tile = 0 if before else chunks
    key_tile = (2 * chunks - 1 if before else chunks - 1) * tile
    size = mid.shape[1]
    for pair in range(len(kvs)):
        kv = kvs[pair]
        for residue in range(FAR_DILATION):
            starts = far_starts(residue, 2 * chunks)
            result = attend(
                rows_of(q, starts, pair_lanes(pair)),
                rows_of(kv, starts, KEYS),
                rows_of(kv, starts, VALUES),
                jnp.concatenate([far[back, 2 * pair], far[back, 2 * pair + 1]], axis=0),
            )
            fold_in(refs, starts, pair_lanes(pair), result)
        result = attend(
            halves(q, query_tile * tile, pair_lanes(pair))[0],
            halves(kv, key_tile, KEYS)[1],
            halves(kv, key_tile, VALUES)[1],
            near_bias(near, pair, 0, slice(0, HALF)),
        )
        for n, rows in enumerate(half_rows(query_tile * tile, 0)):
            where = (rows, pair_lanes(pair))
            piece = tuple(item[n * SUB // 2 : (n + 1) * SUB // 2] for item in result)
            for ref, value in zip(refs, merge(tuple(ref[where] for ref in refs), piece)):
                ref[where] = value
        for residue in range(MIDDLE_DILATION):
            starts = middle_starts(0 if before else 1, residue, chunks)
            key_starts = middle_starts(1 if before else 0, residue, chunks)
            result = attend(
                rows_of(q, starts, pair_lanes(pair)),
                rows_of(kv, key_starts, KEYS),
                rows_of(kv, key_starts, VALUES),
                stacked(mid, pair, slice(0, size), slice(0, size)),
            )
            fold_in(refs, starts, pair_lanes(pair), result)


def pair_kernel(near, mid, far, q_mine, q_part, *rest):
    kv_mine, kv_part, mine, part = rest[:2], rest[2:4], rest[4:7], rest[7:10]
    *refs, q_ref, kv = rest[-5:]
    place_pair(q_ref, q_mine, q_part)
    for n in range(2):
        place_pair(kv.at[n], kv_mine[n], kv_part[n])
    for ref, first, second in zip(refs, mine, part):
        place_pair(ref, first, second)
    windows(refs, q_ref, [kv.at[0], kv.at[1]], near, mid, far, False)


def pair_attention(bias, q_mine, q_part, kv_mine, kv_part, mine, part, after=()):
    block, lanes = q_mine.shape
    return call(
        pair_kernel,
        [((2 * block, lanes), F32)] * 3 + [((2 * block, lanes), BF16)],
        [*bias, q_mine, q_part, *kv_mine, *kv_part, *mine, *part, *after],
        [pltpu.VMEM((2, 2 * block, 256), BF16)],
        limit=16,
        flops=4 * 10**9,
        loose=len(after),
    )


def before_kernel(near, mid, far, q, kv_a0, kv_b0, kv_a1, kv_b1, o_in, m_in, l_in, *rest):
    o_ref, m_ref, l_ref, past = rest[-4:]
    o_ref[...], m_ref[...], l_ref[...] = o_in[...], m_in[...], l_in[...]

    @pl.when(places()[1] > 0)
    def _():
        place_pair(past.at[0], kv_a0, kv_b0)
        place_pair(past.at[1], kv_a1, kv_b1)
        windows((o_ref, m_ref, l_ref), q, [past.at[0], past.at[1]], near, mid, far, True)


def before_attention(bias, q, past, state, after=()):
    return call(
        before_kernel,
        [(q.shape, F32)] * 3,
        [*bias, q, *past, *state, *after],
        [pltpu.VMEM((2, q.shape[0], 256), BF16)],
        limit=16,
        flops=4 * 10**9,
        loose=len(after),
    )


def part_row(shape, block):
    row = lax.broadcasted_iota(jnp.int32, shape, 0) - 8 * block
    lane = lax.broadcasted_iota(jnp.int32, shape, 1)
    return row, lane


def pack_sums(blocks):
    total = 0.0
    for n, sums in enumerate(blocks):
        row, lane = part_row((16, 128), n)
        for part in range(3):
            piece = sums.astype(BF16)
            sums = sums - piece.astype(F32)
            pick = (row // 2 == part) & (row >= 0) & (lane == (row % 2) * HEAD_DIM)
            total = total + lax.dot_general(
                jnp.where(pick, 1.0, 0.0).astype(BF16), piece, (((1,), (1,)), ((), ())), preferred_element_type=F32
            )
    return total.astype(BF16)


def unpack_sums(packed, block):
    row, lane = part_row((16, 128), block)
    pick = (row >= 0) & (row < 6) & (lane // HEAD_DIM == row % 2)
    return lax.dot_general(
        packed, jnp.where(pick, 1.0, 0.0).astype(BF16), (((0,), (0,)), ((), ())), preferred_element_type=F32
    )


def store_packed(ref, first, packed):
    for n in range(packed.shape[1] // 128):
        ref[first + 16 * n : first + 16 * (n + 1)] = packed[:, n * 128 : (n + 1) * 128]


def load_packed(ref, first, count):
    return jnp.concatenate([ref[first + 16 * n : first + 16 * (n + 1)] for n in range(count)], axis=1)


def remote_kernel(pair, far, q_a, q_b, kv_a, kv_b, *rest):
    out_ref, q, kv, sums = rest[-4:]
    block = q_a.shape[0]
    tile = FAR_DILATION * SUB
    chunks = block // tile
    _, z, _ = places()
    useful = (z > 0) & (z + 1 < lax.axis_size("sp") // 2)

    @pl.when(useful)
    def _():
        place_pair(q, q_a.at[:, pair_lanes(pair)], q_b.at[:, pair_lanes(pair)])
        place_pair(kv, kv_a, kv_b)
        bias = jnp.concatenate([far[2, 2 * pair], far[2, 2 * pair + 1]], axis=0)
        for residue in range(FAR_DILATION):
            starts = far_starts(residue, 2 * chunks)
            o, m, l = attend(rows_of(q, starts, KEYS), rows_of(kv, starts, KEYS), rows_of(kv, starts, VALUES), bias)
            some = l > 0.0
            safe = jnp.where(some, l, 1.0)
            o = o / safe
            s = jnp.where(some, m + jnp.log2(safe), FLOOR)
            for n, start in enumerate(starts):
                where = pl.ds(start, SUB)
                out_ref[where] = o[n * SUB : (n + 1) * SUB].astype(BF16)
                sums[where] = s[n * SUB : (n + 1) * SUB]
        store_packed(out_ref, 2 * block, pack_sums([sums[:block], sums[block:]]))

    @pl.when(jnp.logical_not(useful))
    def _():
        out_ref[: 2 * block] = jnp.zeros((2 * block, 128), BF16)
        store_packed(out_ref, 2 * block, pack_sums([jnp.full((block, 128), FLOOR, F32)] * 2))


def remote_attention(pair, far, q_a, q_b, kv_a, kv_b, after=()):
    block = q_a.shape[0]
    return call(
        functools.partial(remote_kernel, pair),
        [((2 * block + 16 * (block // 128), 128), BF16)],
        [far, q_a, q_b, kv_a, kv_b, *after],
        [pltpu.VMEM((2 * block, 128), BF16), pltpu.VMEM((2 * block, 256), BF16), pltpu.VMEM((2 * block, 128), F32)],
        limit=8,
        flops=10**9,
        loose=len(after),
    )[0]


def finish_kernel(pair, o_in, m_in, l_in, far_in, *rest):
    stay_ref, go_ref, same_ref, cross_ref, sums_ref, o_s, turned = rest[-7:]
    y, _, tp = places()
    rows = o_in.shape[0]
    block = rows // 2
    half = block // 2
    tile = FAR_DILATION * SUB
    lanes = pair_lanes(pair)
    closed = closed_gate()
    packed = load_packed(far_in, rows, block // 128)
    for b in range(2):
        far_sums = unpack_sums(packed, b) + closed
        select = slice(b * block, (b + 1) * block)
        o, m, l = merge(
            (o_in[select, lanes], m_in[select, lanes], l_in[select, lanes]),
            (far_in[select].astype(F32), far_sums, jnp.ones_like(far_sums)),
        )
        o_s[0, select] = o / l
        o_s[1, select] = (m + jnp.log2(l)) * LN2
    for item in range(2):
        for s in range(rows // tile):
            for residue in range(FAR_DILATION):
                turned[item, pl.ds(s * tile + residue, SUB, stride=FAR_DILATION), :] = o_s[
                    item, s * tile + residue * SUB : s * tile + (residue + 1) * SUB
                ]
    own, other = y * block, (1 - y) * block
    for ref, start in (
        (stay_ref, own + tp * half),
        (go_ref, own + (1 - tp) * half),
        (same_ref, other + tp * half),
        (cross_ref, other + (1 - tp) * half),
    ):
        ref[:half] = turned[0, pl.ds(aligned(start, half), half), :].astype(BF16)
    sums_ref[...] = pack_sums([turned[1, pl.ds(aligned(own, block), block), :]])
    store_packed(same_ref, half, pack_sums([turned[1, pl.ds(aligned(other, block), block), :]]))


def finish(pair, state, far, after=()):
    rows = state[0].shape[0]
    block, half = rows // 2, rows // 4
    piece = ((half, 128), BF16)
    return call(
        functools.partial(finish_kernel, pair),
        [piece, piece, ((half + 16 * (block // 128), 128), BF16), piece, ((16, block), BF16)],
        [*state, far, *after],
        [pltpu.VMEM((2, rows, 128), F32), pltpu.VMEM((2, rows, 128), F32)],
        limit=8,
        flops=10**9,
        loose=len(after),
    )


def output_kernel(*refs):
    pieces, (w_mine, w_other, out_ref, sums_ref) = (refs[:5], refs[5:10]), refs[10:]
    y, _, _ = places()
    half, width = out_ref.shape
    block = 2 * half
    low = y == 0
    order = lambda mine, part: (jnp.where(low, mine, part), jnp.where(low, part, mine))
    hidden = []
    for first, second in ((0, 1), (2, 3)):
        blocks = []
        for piece in pieces:
            blocks += order(piece[first][:half], piece[second][:half])
        hidden.append(jnp.concatenate(blocks, axis=1))
    step = 512
    for start in range(0, width, step):
        columns = slice(start, start + step)
        first = jnp.dot(hidden[0], w_mine[:, columns], preferred_element_type=F32)
        second = jnp.dot(hidden[1], w_other[:, columns], preferred_element_type=F32)
        out_ref[:, columns] = (first.astype(BF16).astype(F32) + second.astype(BF16).astype(F32)).astype(BF16)
    heads = []
    for piece in pieces:
        sums = []
        for packed in (piece[4][...], load_packed(piece[1], half, block // 128)):
            packed = packed.astype(F32)
            sums.append(packed[0:2] + packed[2:4] + packed[4:6])
        heads += order(*sums)
    sums_ref[...] = jnp.concatenate(heads, axis=0)


def output(pieces, w_mine, w_other):
    half = pieces[0][0].shape[0]
    width = w_mine.shape[1]
    return call(
        output_kernel,
        [((half, width), BF16), ((8, 2 * half), F32)],
        [*pieces[0], *pieces[1], w_mine, w_other],
        limit=12,
        flops=2 * half * width * 1024,
    )


def layer(tokens, w_query, w_key, w_value, w_out):
    half, _ = tokens.shape
    block = 2 * half
    width = w_query.shape[1]
    heads = width // 2 // HEAD_DIM
    count = lax.axis_size("sp")
    assert lax.axis_size("tp") == 2 and count % 2 == 0
    assert REACH == 4 * block and half == FAR_DILATION * SUB and width == 512
    ahead = [(n, (n + 2) % count) for n in range(count)]
    back = [(n + 2, n) for n in range(count - 2)]
    onward = [(n, n + 2) for n in range(count - 2)]
    beside = [(n, n ^ 1) for n in range(count)]
    swap = [(0, 1), (1, 0)]
    crossed = [(2 * n + c, 2 * (n ^ 1) + 1 - c) for n in range(count) for c in range(2)]

    x_other = lax.ppermute(tokens, "tp", swap)
    kv_t0, kv_m0 = project(tokens, x_other, [w_key[:, :256], w_value[:, :256]], [0])
    kv_p0 = lax.ppermute(kv_t0, "sp", beside)
    kv_a0 = lax.ppermute(kv_m0, "sp", ahead)
    q_t, q_m = project(tokens, x_other, [w_query], [0, 256])
    q_p = lax.ppermute(q_t, "sp", beside)
    q_a = lax.ppermute(q_m, "sp", back)
    kv_t1, kv_m1 = project(tokens, x_other, [w_key, w_value], [256])
    kv_p1 = lax.ppermute(kv_t1, "sp", beside)
    kv_a1 = lax.ppermute(kv_m1, "sp", ahead)
    kv_b0 = lax.ppermute(kv_p0, "sp", onward)
    q_b = lax.ppermute(q_p, "sp", back)
    kv_b1 = lax.ppermute(kv_p1, "sp", onward)
    w_other = lax.ppermute(w_out, "tp", swap)
    bias = biases(block, heads)
    mine = block_attention(bias, q_m, kv_m0, kv_m1)
    part = block_attention(bias, q_p, kv_p0, kv_p1, mine[:1])
    far0 = remote_attention(0, bias[2], q_a, q_b, kv_a0, kv_b0)
    far_p = lax.ppermute(far0, "sp", ahead)
    *state, q = pair_attention(bias, q_m, q_p, (kv_m0, kv_m1), (kv_p0, kv_p1), mine, part)
    far1 = remote_attention(1, bias[2], q_a, q_b, kv_a1, kv_b1)
    far_m = lax.ppermute(far1, "sp", onward)
    state = before_attention(bias, q, (kv_a0, kv_b0, kv_a1, kv_b1), state)
    pieces = []
    for pair, far in enumerate((far_p, far_m)):
        stay, go, same, cross, sums = finish(pair, state, far)
        same = lax.ppermute(same, "sp", beside)
        cross = lax.ppermute(cross, ("sp", "tp"), crossed)
        go = lax.ppermute(go, "tp", swap)
        pieces.append((stay, same, go, cross, sums))
    return output(pieces, w_out, w_other)


def solution(mesh):
    in_specs = (
        P(("grp", "sp", "tp"), None),
        P(None, "tp"),
        P(None, "tp"),
        P(None, "tp"),
        P("tp", None),
    )
    out_specs = (P(("grp", "sp", "tp"), None), P("tp", ("grp", "sp")))
    return jax.shard_map(layer, mesh=mesh, in_specs=in_specs, out_specs=out_specs, check_vma=False)
```
